256 devices in a mesh: sp: 64 (over z, x, core), tp: 4 (over y).
Axes of the slice: x: 4, y: 4, z: 8, core: 2. Of those that a mesh axis runs over, the one named last changes fastest.
Arguments:
- resid: bfloat16 [16384, 4096], P(('sp', 'tp')), may hold values from -6 to 6
- queries: bfloat16 [16384, 2048], P('sp', 'tp'), may hold values from -6 to 6
- keys: bfloat16 [16384, 512], P('sp', 'tp'), may hold values from -6 to 6
- values: bfloat16 [16384, 512], P('sp', 'tp'), may hold values from -6 to 6
- q_gain: float32 [128], replicated, may hold values from 0.5 to 6
- key_norm_gain: float32 [128], replicated, may hold values from 0.5 to 6
- out_weight: bfloat16 [2048, 4096], P('tp'), may hold values from -0.125 to 0.125
- norm1_gain: float32 [4096], replicated, may hold values from 0.1 to 1.9
- norm2_gain: float32 [4096], replicated, may hold values from 0.1 to 1.9
- expert_ids: int32 [16384, 2], P(('sp', 'tp')), may hold values from 0 to 63, all different within a row; in each aligned block of 64 rows (0 to 63, 64 to 127, ...) at most 3 rows name the same one
- group_weight: float32 [16384], P(('sp', 'tp')), may hold values from 0.3 to 1
- expert_weight: float32 [16384, 2], P(('sp', 'tp')), may hold values from 0.1 to 1
- gate_proj: bfloat16 [64, 4096, 1024], P('sp', None, 'tp'), may hold values from -0.09375 to 0.09375
- up_proj: bfloat16 [64, 4096, 1024], P('sp', None, 'tp'), may hold values from -0.09375 to 0.09375
- down_proj: bfloat16 [64, 1024, 4096], P('sp', 'tp'), may hold values from -0.1875 to 0.1875
Outputs:
- mixed_out: bfloat16 [16384, 4096], P(('sp', 'tp'))
The draws below stay inside these ranges and needn't reach their ends.
Inputs may be any that keep to these rules, and one draw needn't show every extreme that they name: `expert_ids`: each row names 2 different experts. Among the rows of one device (aligned blocks of 64 rows) no expert is named by more than 3 rows, a bound that some block reaches.
All inputs are finite; a program needn't handle non-finite values.
Results may differ from the reference program's by a relative error of at most 0.012.
The reference program's roundings to bfloat16 on the way count: a program that leaves them out, or rounds other values in their place, can miss the bound.
Values may be sent and summed in bfloat16 or wider, within the bound.
A program may use at most 192 MiB of HBM per device.

```python
import math
import jax
import jax.numpy as jnp
import numpy as np
from jax import lax

D = 4096
HEAD_WIDTH = 128
QUERY_HEADS = 16
KEY_VALUE_HEADS = 4
GRID_W = 64
FF = 1024
TOP = 2
SEQUENCE_TOKENS = 16384
ROWS_DEV = 64
EXPERTS = 64
CAP = 3
N_SP = 64
N_TP = 4


def gain_law(key):
    return jax.random.uniform(key, (HEAD_WIDTH,), jnp.float32, 0.5, 2.0)


def draw_q_gain(key, part):
    return gain_law(jax.random.fold_in(key, 31))


def draw_key_norm_gain(key, part):
    return gain_law(jax.random.fold_in(key, 37))


def key_table(key):
    sampled_values = jax.random.normal(jax.random.fold_in(key, 41), (SEQUENCE_TOKENS, KEY_VALUE_HEADS * HEAD_WIDTH), jnp.float32)
    return jnp.clip(sampled_values, -6.0, 6.0)


def draw_keys(key, part):
    return key_table(key).astype(jnp.bfloat16)


def draw_queries(key, part):
    sampled_values = jax.random.normal(jax.random.fold_in(key, 43), (SEQUENCE_TOKENS, QUERY_HEADS * HEAD_WIDTH), jnp.float32)
    sampled_values = jnp.clip(sampled_values, -6.0, 6.0)
    return sampled_values.astype(jnp.bfloat16)


def block_scale(stream_key, shape, split, low, high):
    def one(dim, parts):
        draws = jax.random.uniform(jax.random.fold_in(jax.random.fold_in(stream_key, 6), dim), (parts,), jnp.float32, low / len(split), high / len(split))
        return jnp.repeat(jnp.exp(draws), shape[dim] // parts).reshape((-1,) + (1,) * (len(shape) - dim - 1))

    loudness = one(*split[0])
    for cut in split[1:]:
        loudness = loudness * one(*cut)
    return loudness


def routed_block(own_key, own, number, rows, amount, top, reach, lean):
    ranking = jax.random.permutation(own_key, amount)
    heavy_load, common = load_shares(amount, rows * top, reach, lean, True), load_shares(amount, rows * top, reach, lean, False)
    places = jnp.arange(amount)

    def named(tallies, turn):
        used = int((tallies > 0).sum())
        fixed = max(1, used // 4)
        shifted = fixed + (places - fixed + turn * (used - fixed)) % max(1, amount - fixed)
        return jnp.zeros((amount,), jnp.int32).at[ranking[jnp.where(places < fixed, places, shifted)]].set(jnp.asarray(tallies, jnp.int32))

    tallies = jnp.where(number % 4 == 0, named(heavy_load, number // 4), named(common, number - number // 4 - 1))
    mixed = jax.random.permutation(jax.random.fold_in(own, 3), amount)
    donor, sink = mixed[0:amount // 2 * 2:2], mixed[1:amount // 2 * 2:2]
    slack = jnp.minimum(tallies[donor] - 1, reach - tallies[sink]) // 2
    slack = jnp.where((donor == ranking[0]) | (sink == ranking[0]) | (tallies[sink] == 0), 0, jnp.maximum(slack, 0))
    shifted = jax.random.randint(jax.random.fold_in(own, 4), (amount // 2,), 0, 1 << 20) % (slack + 1)
    tallies = tallies.at[donor].add(-shifted).at[sink].add(shifted)
    items = jnp.searchsorted(jnp.cumsum(tallies), jnp.arange(rows * top), side="right").astype(jnp.int32)
    table = items.reshape(top, rows).T
    table = table[jax.random.permutation(jax.random.fold_in(own, 1), rows)]
    turn = jax.random.randint(jax.random.fold_in(own, 2), (rows, 1), 0, top)
    return jnp.take_along_axis(table, (jnp.arange(top)[None, :] + turn) % top, axis=1)


def load_shares(count, total, bound, skew, full):
    weights = [(1 << 20) // math.isqrt(grade ** skew) + 1 for grade in range(1, count + 1)]
    largest = bound if full else min(bound, max(-(-total // count), total * weights[0] // sum(weights)))
    least = 1 if total - largest >= count - 1 else 0
    holding, surplus = [largest] + [least] * (count - 1), total - largest - least * (count - 1)
    while surplus > 0:
        free = [i for i in range(1, count) if holding[i] < largest] or [i for i in range(1, count) if holding[i] < bound]
        whole, left = sum([weights[i] for i in free]), surplus
        for i in free:
            more = min(bound - holding[i], max(1, left * weights[i] // whole), surplus)
            holding[i] = holding[i] + more
            surplus = surplus - more
    return np.array(holding)


def normal_values(rng, dims, deviation, bound, split=(), kind=jnp.bfloat16):
    values = deviation * jax.random.normal(rng, dims, jnp.float32)
    if split:
        values = values * block_scale(rng, dims, split, -0.22, 0.18)
    return jnp.clip(values, -bound, bound).astype(kind)


def setup_inputs(seed: int = 0) -> dict:
    streams_of = jax.random.split(jax.random.key(seed), 16)
    resid = normal_values(streams_of[0], (SEQUENCE_TOKENS, D), 1.0, 6.0, ((0, 256),))
    queries = draw_queries(jax.random.fold_in(streams_of[15], 71), 0)
    keys = draw_keys(jax.random.fold_in(streams_of[15], 71), 0)
    values = normal_values(streams_of[3], (SEQUENCE_TOKENS, KEY_VALUE_HEADS * HEAD_WIDTH), 1.0, 6.0, ((0, 64), (1, 4)))
    q_gain = draw_q_gain(jax.random.fold_in(streams_of[15], 71), 0)
    key_norm_gain = draw_key_norm_gain(jax.random.fold_in(streams_of[15], 71), 0)
    out_weight = normal_values(streams_of[6], (QUERY_HEADS * HEAD_WIDTH, D), (QUERY_HEADS * HEAD_WIDTH) ** -0.5, 0.125, ((0, 4),))
    norm1_gain = jnp.clip(1.0 + 0.18 * jax.random.normal(streams_of[7], (D,), jnp.float32), 0.1, 1.9)
    norm2_gain = jnp.clip(1.0 + 0.18 * jax.random.normal(streams_of[8], (D,), jnp.float32), 0.1, 1.9)
    expert_ids_keys = jax.random.split(jax.random.fold_in(streams_of[9], 1), SEQUENCE_TOKENS // ROWS_DEV)
    expert_ids_turns = jax.random.permutation(jax.random.fold_in(streams_of[9], 3), SEQUENCE_TOKENS // ROWS_DEV)
    expert_ids = jax.vmap(lambda own, number: routed_block(jax.random.fold_in(streams_of[9], 2), own, number, ROWS_DEV, EXPERTS, TOP, CAP, 1))(expert_ids_keys, expert_ids_turns).reshape((SEQUENCE_TOKENS, TOP))
    group_weight = jnp.clip(0.3 + 0.7 * jax.random.uniform(streams_of[10], (SEQUENCE_TOKENS,), jnp.float32) ** block_scale(streams_of[10], (SEQUENCE_TOKENS,), ((0, 256),), -0.2, 0.2), 0.3, 1.0)
    expert_weight = jnp.clip(0.1 + 0.9 * jax.random.uniform(streams_of[11], (SEQUENCE_TOKENS, TOP), jnp.float32) ** block_scale(streams_of[11], (SEQUENCE_TOKENS, TOP), ((0, 256),), -0.2, 0.2), 0.1, 1.0)
    gate_proj = normal_values(streams_of[12], (EXPERTS, D, FF), D ** -0.5, 0.09375, ((0, 64), (2, 4)))
    up_proj = normal_values(streams_of[13], (EXPERTS, D, FF), D ** -0.5, 0.09375, ((0, 64), (2, 4)))
    down_proj = normal_values(streams_of[14], (EXPERTS, FF, D), FF ** -0.5, 0.1875, ((0, 64), (1, 4)))
    return dict(resid=resid, queries=queries, keys=keys, values=values, q_gain=q_gain, key_norm_gain=key_norm_gain, out_weight=out_weight, norm1_gain=norm1_gain, norm2_gain=norm2_gain, expert_ids=expert_ids, group_weight=group_weight, expert_weight=expert_weight, gate_proj=gate_proj, up_proj=up_proj, down_proj=down_proj)


deep_alpha = 2.0 ** 0.5
rope_theta = 10000.0

def apply_rotary_heads(block, gain, grid_positions):
    values32 = block.astype(jnp.float32)
    normed = values32 * lax.rsqrt(lax.optimization_barrier(jnp.mean(values32 * values32, -1, keepdims=True)) + 1e-06) * gain
    half = normed.shape[-1] // 2
    inv_freq = rope_theta ** (-jnp.arange(0, half, 2, dtype=jnp.float32) / half)
    grid_row = (grid_positions // GRID_W).astype(jnp.float32)
    grid_col = (grid_positions % GRID_W).astype(jnp.float32)
    angle = jnp.concatenate([grid_row[:, None] * inv_freq, grid_col[:, None] * inv_freq], -1)[:, None, :]
    cosine = jnp.cos(angle)
    sine = jnp.sin(angle)
    first = normed[..., :half]
    second = normed[..., half:]
    turned = jnp.concatenate([first * cosine - second * sine, first * sine + second * cosine], -1)
    return turned.astype(jnp.bfloat16)

def layer_norm_gain(summed, gain):
    centre = summed - lax.optimization_barrier(jnp.mean(summed, -1, keepdims=True))
    spread = lax.optimization_barrier(jnp.mean(centre * centre, -1, keepdims=True))
    return centre * lax.rsqrt(spread + 1e-06) * gain

def reference(resid, queries, keys, values, q_gain, key_norm_gain, out_weight, norm1_gain, norm2_gain, expert_ids, group_weight, expert_weight, gate_proj, up_proj, down_proj):
    grid_positions = jnp.arange(SEQUENCE_TOKENS, dtype=jnp.int32)
    query_group = QUERY_HEADS // KEY_VALUE_HEADS
    q_rot = apply_rotary_heads(queries.reshape(SEQUENCE_TOKENS, QUERY_HEADS, HEAD_WIDTH), q_gain, grid_positions)
    rotated_keys = apply_rotary_heads(keys.reshape(SEQUENCE_TOKENS, KEY_VALUE_HEADS, HEAD_WIDTH), key_norm_gain, grid_positions).astype(jnp.float32)
    value_rows_full = values.reshape(SEQUENCE_TOKENS, KEY_VALUE_HEADS, HEAD_WIDTH).astype(jnp.float32)
    query_extent = math.gcd(SEQUENCE_TOKENS, 128)

    def attend(query_tile):
        query_widened = query_tile.reshape(query_extent, KEY_VALUE_HEADS, query_group, HEAD_WIDTH).astype(jnp.float32)
        scores = jnp.einsum('qkgd,lkd->kgql', query_widened, rotated_keys) * HEAD_WIDTH ** (-0.5)
        row_max = lax.optimization_barrier(jnp.max(scores, -1, keepdims=True))
        weights = jnp.exp(scores - row_max)
        row_sum = lax.optimization_barrier(jnp.sum(weights, -1))
        rounded = lax.optimization_barrier(weights.astype(jnp.bfloat16)).astype(jnp.float32)
        mixed = jnp.einsum('kgql,lkd->qkgd', rounded, value_rows_full)
        mixed = mixed / jnp.transpose(row_sum, (2, 0, 1))[..., None]
        return mixed.reshape(query_extent, QUERY_HEADS * HEAD_WIDTH).astype(jnp.bfloat16)
    attn = lax.map(attend, q_rot.reshape(SEQUENCE_TOKENS // query_extent, query_extent, QUERY_HEADS, HEAD_WIDTH)).reshape(SEQUENCE_TOKENS, QUERY_HEADS * HEAD_WIDTH)
    proj = jnp.dot(attn, out_weight, preferred_element_type=jnp.float32).astype(jnp.bfloat16)
    summed = deep_alpha * resid.astype(jnp.float32) + proj.astype(jnp.float32)
    x_one = layer_norm_gain(summed, norm1_gain).astype(jnp.bfloat16)
    gates = group_weight[:, None] * expert_weight / lax.optimization_barrier(jnp.sum(expert_weight, -1, keepdims=True))
    copies = SEQUENCE_TOKENS * TOP
    most_rows = CAP * N_SP * N_TP
    ff_dev = FF // N_TP
    flat_ids = expert_ids.reshape(-1)
    gate_flat = jnp.concatenate([gates.reshape(-1), jnp.zeros((1,), jnp.float32)])
    x_padded = jnp.concatenate([x_one, jnp.zeros((1, D), jnp.bfloat16)], 0)

    def per_expert(total, expert):
        index = jnp.nonzero(flat_ids == expert, size=most_rows, fill_value=copies)[0].astype(jnp.int32)
        token_index = jnp.where(index < copies, index // TOP, SEQUENCE_TOKENS).astype(jnp.int32)
        chosen = x_padded[token_index]
        w_gate = lax.dynamic_index_in_dim(gate_proj, expert, 0, keepdims=False)
        w_up = lax.dynamic_index_in_dim(up_proj, expert, 0, keepdims=False)
        w_down = lax.dynamic_index_in_dim(down_proj, expert, 0, keepdims=False)
        gate_part = jnp.dot(chosen, w_gate, preferred_element_type=jnp.float32)
        up_part = jnp.dot(chosen, w_up, preferred_element_type=jnp.float32)
        hidden = (jax.nn.silu(gate_part) * up_part).astype(jnp.bfloat16)
        expert_sum = jnp.zeros((most_rows, D), jnp.float32)
        for lane in range(N_TP):
            partial_sum = jnp.dot(hidden[:, lane * ff_dev:(lane + 1) * ff_dev], w_down[lane * ff_dev:(lane + 1) * ff_dev], preferred_element_type=jnp.float32)
            rounded = lax.optimization_barrier(partial_sum.astype(jnp.bfloat16))
            expert_sum = expert_sum + rounded.astype(jnp.float32)
        expert_out = expert_sum.astype(jnp.bfloat16).astype(jnp.float32)
        weighted = gate_flat[index][:, None] * expert_out
        return (total.at[token_index].add(weighted), None)
    start_total = jnp.zeros((SEQUENCE_TOKENS + 1, D), jnp.float32)
    moe_total, _ = lax.scan(per_expert, start_total, jnp.arange(EXPERTS, dtype=jnp.int32))
    moe = moe_total[:SEQUENCE_TOKENS]
    final = deep_alpha * x_one.astype(jnp.float32) + moe
    return layer_norm_gain(final, norm2_gain).astype(jnp.bfloat16)
```

```python
import jax
import jax.numpy as jnp
import numpy as np
from jax import lax
from jax.experimental import pallas as pl
from jax.experimental.pallas import tpu as pltpu
from jax.sharding import PartitionSpec as P

GRID_W = 64
CAP = 3
KEY_BLOCK = 1024
QUERY_TILE = 512

deep_alpha = 2.0**0.5
rope_theta = 10000.0
VMEM_LIMIT = 60 * 1024 * 1024


def apply_rotary_heads(block, gain, grid_positions):
    values32 = block.astype(jnp.float32)
    normed = values32 * lax.rsqrt(jnp.mean(values32 * values32, -1, keepdims=True) + 1e-06) * gain
    half = normed.shape[-1] // 2
    inv_freq = rope_theta ** (-jnp.arange(0, half, 2, dtype=jnp.float32) / half)
    grid_row = (grid_positions // GRID_W).astype(jnp.float32)
    grid_col = (grid_positions % GRID_W).astype(jnp.float32)
    angle = jnp.concatenate([grid_row[:, None] * inv_freq, grid_col[:, None] * inv_freq], -1)[
        :, None, :
    ]
    cosine = jnp.cos(angle)
    sine = jnp.sin(angle)
    first = normed[..., :half]
    second = normed[..., half:]
    turned = jnp.concatenate([first * cosine - second * sine, first * sine + second * cosine], -1)
    return turned.astype(jnp.bfloat16)


def attention_kernel(qt_ref, k_ref, v_ref, o_ref, m_ref, l_ref, acc_ref):
    step = pl.program_id(0)
    rows = qt_ref.shape[1]
    width = v_ref.shape[1]
    heads = o_ref.shape[1] // width
    tokens = o_ref.shape[0]

    @pl.when(step == 0)
    def _():
        m_ref[...] = jnp.full_like(m_ref, -1e30)
        l_ref[...] = jnp.zeros_like(l_ref)
        acc_ref[...] = jnp.zeros_like(acc_ref)

    k = k_ref[...]
    k_twice = jnp.concatenate([k, k], 1)
    v_t = v_ref[...].T
    tile = min(QUERY_TILE, rows)
    count = rows // tile

    def scores(t):
        return jnp.dot(
            k_twice, qt_ref[:, t * tile : (t + 1) * tile], preferred_element_type=jnp.float32
        )

    s = scores(0)
    for t in range(count):
        following = scores(t + 1) if t + 1 < count else None
        at = slice(t * tile, (t + 1) * tile)
        m_old = m_ref[:, at]
        m_new = jnp.maximum(m_old, jnp.max(s, 0, keepdims=True))
        shrink = jnp.exp2(m_old - m_new)
        p = jnp.exp2(s - m_new)
        l_ref[:, at] = l_ref[:, at] * shrink + jnp.sum(p, 0, keepdims=True)
        m_ref[:, at] = m_new
        pv = jnp.dot(v_t, p.astype(jnp.bfloat16), preferred_element_type=jnp.float32)
        acc_ref[:, at] = acc_ref[:, at] * shrink + pv
        s = following

    @pl.when(step == pl.num_programs(0) - 1)
    def _():
        for h in range(heads):
            at = slice(h * tokens, (h + 1) * tokens)
            out = acc_ref[:, at] / l_ref[:, at]
            o_ref[:, h * width : (h + 1) * width] = out.T.astype(jnp.bfloat16)


def attention(q_t, keys_values, tokens, width):
    length = keys_values.shape[0]
    rows = q_t.shape[1]
    block = min(KEY_BLOCK, length)
    heads = rows // tokens
    return pl.pallas_call(
        attention_kernel,
        grid=(length // block,),
        in_specs=[
            pl.BlockSpec(q_t.shape, lambda i: (0, 0)),
            pl.BlockSpec((block, width), lambda i: (i, 0)),
            pl.BlockSpec((block, width), lambda i: (i, 1)),
        ],
        out_specs=pl.BlockSpec((tokens, heads * width), lambda i: (0, 0)),
        out_shape=jax.ShapeDtypeStruct((tokens, heads * width), jnp.bfloat16),
        scratch_shapes=[
            pltpu.VMEM((1, rows), jnp.float32),
            pltpu.VMEM((1, rows), jnp.float32),
            pltpu.VMEM((width, rows), jnp.float32),
        ],
        compiler_params=pltpu.CompilerParams(vmem_limit_bytes=VMEM_LIMIT),
        cost_estimate=pl.CostEstimate(
            flops=4 * rows * length * width,
            bytes_accessed=length * width * 4,
            transcendentals=rows * length,
        ),
        name="attention",
    )(q_t, keys_values, keys_values)


def gate_up_kernel(x_ref, wg_ref, wu_ref, h_ref):
    parts, _, depth = x_ref.shape
    gate = None
    up = None
    for j in range(parts):
        x = x_ref[j]
        g = jnp.dot(x, wg_ref[j * depth : (j + 1) * depth, :], preferred_element_type=jnp.float32)
        u = jnp.dot(x, wu_ref[j * depth : (j + 1) * depth, :], preferred_element_type=jnp.float32)
        gate = g if gate is None else gate + g
        up = u if up is None else up + u
    h_ref[...] = (gate / (1.0 + jnp.exp(-gate)) * up).astype(jnp.bfloat16)


def gate_up(x, w_gate, w_up):
    parts, rows, depth = x.shape
    hidden = w_gate.shape[1]
    block = rows // 4
    return pl.pallas_call(
        gate_up_kernel,
        grid=(rows // block,),
        in_specs=[
            pl.BlockSpec((parts, block, depth), lambda i: (0, i, 0)),
            pl.BlockSpec(w_gate.shape, lambda i: (0, 0)),
            pl.BlockSpec(w_up.shape, lambda i: (0, 0)),
        ],
        out_specs=pl.BlockSpec((block, hidden), lambda i: (i, 0)),
        out_shape=jax.ShapeDtypeStruct((rows, hidden), jnp.bfloat16),
        compiler_params=pltpu.CompilerParams(vmem_limit_bytes=VMEM_LIMIT),
        cost_estimate=pl.CostEstimate(
            flops=4 * rows * parts * depth * hidden,
            bytes_accessed=2 * parts * depth * (rows + 2 * hidden),
            transcendentals=rows * hidden,
        ),
        name="gate_up",
    )(x, w_gate, w_up)


def down_kernel(h_ref, w_ref, o_ref):
    parts, _, depth = h_ref.shape
    total = None
    for j in range(parts):
        part = jnp.dot(
            h_ref[j], w_ref[j * depth : (j + 1) * depth, :], preferred_element_type=jnp.float32
        )
        part = part.astype(jnp.bfloat16).astype(jnp.float32)
        total = part if total is None else total + part
    o_ref[...] = total.astype(jnp.bfloat16)


def down(h, w):
    parts, rows, depth = h.shape
    width = w.shape[1]
    block = rows // 4
    return pl.pallas_call(
        down_kernel,
        grid=(rows // block,),
        in_specs=[
            pl.BlockSpec((parts, block, depth), lambda i: (0, i, 0)),
            pl.BlockSpec(w.shape, lambda i: (0, 0)),
        ],
        out_specs=pl.BlockSpec((block, width), lambda i: (i, 0)),
        out_shape=jax.ShapeDtypeStruct((rows, width), jnp.bfloat16),
        compiler_params=pltpu.CompilerParams(vmem_limit_bytes=VMEM_LIMIT),
        cost_estimate=pl.CostEstimate(
            flops=2 * rows * parts * depth * width,
            bytes_accessed=2 * parts * depth * (rows + width) + 2 * rows * width,
            transcendentals=0,
        ),
        name="down",
    )(h, w)


def split_layer_norm(z, gain):
    local = z.shape[-1]
    mean = jnp.mean(z, -1)
    centre = z - mean[:, None]
    m2 = jnp.sum(centre * centre, -1)
    both = lax.all_gather(jnp.stack([mean, m2]), "tp", axis=0, tiled=False)
    means, m2s = both[:, 0], both[:, 1]
    full_mean = jnp.mean(means, 0)
    away = means - full_mean[None]
    spread = (jnp.sum(m2s, 0) + local * jnp.sum(away * away, 0)) / (local * both.shape[0])
    return (z - full_mean[:, None]) * lax.rsqrt(spread + 1e-06)[:, None] * gain


def per_device(
    resid,
    queries,
    keys,
    values,
    q_gain,
    key_norm_gain,
    out_weight,
    norm1_gain,
    norm2_gain,
    expert_ids,
    group_weight,
    expert_weight,
    gate_proj,
    up_proj,
    down_proj,
):
    tokens = queries.shape[0]
    width = q_gain.shape[0]
    heads = queries.shape[1] // width
    lanes = lax.axis_size("tp")
    sp_count = lax.axis_size("sp")
    lane = lax.axis_index("tp")
    own = tokens // lanes
    model_width = resid.shape[1]
    part = model_width // lanes

    positions = lax.axis_index("sp") * tokens + jnp.arange(tokens, dtype=jnp.int32)
    rotated_keys = apply_rotary_heads(keys.reshape(tokens, 1, width), key_norm_gain, positions)
    both = jnp.concatenate([rotated_keys.reshape(tokens, width), values], 1)
    keys_values = lax.all_gather(both, "sp", axis=0, tiled=True)

    out_slice = lax.all_to_all(out_weight, "tp", split_axis=1, concat_axis=0, tiled=True)
    down_slice = lax.all_to_all(down_proj[0], "tp", split_axis=1, concat_axis=0, tiled=True)
    resid_slice = lax.all_to_all(resid, "tp", split_axis=1, concat_axis=0, tiled=True)
    ids = lax.all_gather(expert_ids, "tp", axis=0, tiled=True)
    gates_own = (
        group_weight[:, None] * expert_weight / jnp.sum(expert_weight, -1, keepdims=True)
    )
    gates = lax.all_gather(gates_own, "tp", axis=0, tiled=True)

    q_rot = apply_rotary_heads(queries.reshape(tokens, heads, width), q_gain, positions)
    factor = np.float32(np.log2(np.e) * width**-0.5)
    scaled = q_rot.astype(jnp.float32) * factor
    coarse = lax.reduce_precision(scaled, 8, 7)
    fine = (scaled - coarse).astype(jnp.bfloat16)
    pair = jnp.concatenate([coarse.astype(jnp.bfloat16), fine], -1)
    q_t = pair.transpose(2, 1, 0).reshape(2 * width, heads * tokens)
    attn = attention(q_t, keys_values, tokens, width)
    attn = lax.all_gather(attn, "tp", axis=1, tiled=True)

    proj = jnp.dot(attn, out_slice, preferred_element_type=jnp.float32)
    proj = lax.reduce_precision(proj, 8, 7)
    summed = deep_alpha * resid_slice.astype(jnp.float32) + proj
    gain_one = lax.dynamic_slice_in_dim(norm1_gain, lane * part, part)
    gain_two = lax.dynamic_slice_in_dim(norm2_gain, lane * part, part)
    x_one = split_layer_norm(summed, gain_one).astype(jnp.bfloat16)

    top = ids.shape[1]
    per_expert = lanes * CAP
    blocks = ids.reshape(lanes, own * top)
    one_hot = (blocks[:, :, None] == jnp.arange(sp_count, dtype=jnp.int32)).astype(jnp.int32)
    earlier = jnp.cumsum(one_hot, 1) - one_hot
    rank = jnp.sum(earlier * one_hot, 2)
    slot = blocks * per_expert + jnp.arange(lanes, dtype=jnp.int32)[:, None] * CAP + rank
    slot = slot.reshape(tokens, top)
    slots = sp_count * per_expert
    chosen = slot[:, :, None] == jnp.arange(slots, dtype=jnp.int32)
    placing = jnp.any(chosen, 1).astype(jnp.bfloat16)
    outgoing = lax.dot_general(
        placing, x_one, (((0,), (0,)), ((), ())), preferred_element_type=jnp.float32
    ).astype(jnp.bfloat16)
    received = lax.all_to_all(
        outgoing.reshape(sp_count, per_expert, part), "sp", split_axis=0, concat_axis=0, tiled=True
    )
    gathered = lax.all_gather(received.reshape(slots, part), "tp", axis=0, tiled=False)
    hidden = gate_up(gathered, gate_proj[0], up_proj[0])
    hidden = lax.all_gather(hidden, "tp", axis=0, tiled=False)
    expert_out = down(hidden, down_slice)
    returned = lax.all_to_all(
        expert_out.reshape(sp_count, per_expert, part),
        "sp",
        split_axis=0,
        concat_axis=0,
        tiled=True,
    ).reshape(slots, part)
    weights = jnp.sum(jnp.where(chosen, gates[:, :, None], 0.0), 1)
    moe = None
    for _ in range(3):
        term = lax.reduce_precision(weights, 8, 7)
        weights = weights - term
        piece = jnp.dot(
            term.astype(jnp.bfloat16), returned, preferred_element_type=jnp.float32
        )
        moe = piece if moe is None else moe + piece
    final = deep_alpha * x_one.astype(jnp.float32) + moe
    mixed = split_layer_norm(final, gain_two).astype(jnp.bfloat16)
    return lax.all_to_all(mixed, "tp", split_axis=0, concat_axis=1, tiled=True)


def solution(mesh):
    in_specs = (
        P(("sp", "tp"), None),
        P("sp", "tp"),
        P("sp", "tp"),
        P("sp", "tp"),
        P(),
        P(),
        P("tp", None),
        P(),
        P(),
        P(("sp", "tp"), None),
        P(("sp", "tp")),
        P(("sp", "tp"), None),
        P("sp", None, "tp"),
        P("sp", None, "tp"),
        P("sp", "tp", None),
    )
    out_specs = P(("sp", "tp"), None)
    return jax.shard_map(
        per_device, mesh=mesh, in_specs=in_specs, out_specs=out_specs, check_vma=False
    )
```

```python
import jax
import jax.numpy as jnp
import numpy as np
from jax import lax
from jax.experimental import pallas as pl
from jax.experimental.pallas import tpu as pltpu
from jax.sharding import PartitionSpec as P

GRID_W = 64
CAP = 3
KEY_BLOCK = 1024
QUERY_TILE = 512

deep_alpha = 2.0**0.5
rope_theta = 10000.0
VMEM_LIMIT = 60 * 1024 * 1024
MESH = pl.DeviceIdType.MESH
Z_SIZE = 8
X_SIZE = 4
LANES = 4


def apply_rotary_heads(block, gain, grid_positions):
    values32 = block.astype(jnp.float32)
    normed = values32 * lax.rsqrt(jnp.mean(values32 * values32, -1, keepdims=True) + 1e-06) * gain
    half = normed.shape[-1] // 2
    inv_freq = rope_theta ** (-jnp.arange(0, half, 2, dtype=jnp.float32) / half)
    grid_row = (grid_positions // GRID_W).astype(jnp.float32)
    grid_col = (grid_positions % GRID_W).astype(jnp.float32)
    angle = jnp.concatenate([grid_row[:, None] * inv_freq, grid_col[:, None] * inv_freq], -1)[
        :, None, :
    ]
    cosine = jnp.cos(angle)
    sine = jnp.sin(angle)
    first = normed[..., :half]
    second = normed[..., half:]
    turned = jnp.concatenate([first * cosine - second * sine, first * sine + second * cosine], -1)
    return turned.astype(jnp.bfloat16)


def attention_kernel(qt_ref, k_ref, v_ref, o_ref, m_ref, l_ref, acc_ref):
    step = pl.program_id(0)
    rows = qt_ref.shape[1]
    width = v_ref.shape[1]
    heads = o_ref.shape[1] // width
    tokens = o_ref.shape[0]

    @pl.when(step == 0)
    def _():
        m_ref[...] = jnp.full_like(m_ref, -1e30)
        l_ref[...] = jnp.zeros_like(l_ref)
        acc_ref[...] = jnp.zeros_like(acc_ref)

    k = k_ref[...]
    k_twice = jnp.concatenate([k, k], 1)
    v_t = v_ref[...].T
    tile = min(QUERY_TILE, rows)
    count = rows // tile

    def scores(t):
        return jnp.dot(
            k_twice, qt_ref[:, t * tile : (t + 1) * tile], preferred_element_type=jnp.float32
        )

    s = scores(0)
    for t in range(count):
        following = scores(t + 1) if t + 1 < count else None
        at = slice(t * tile, (t + 1) * tile)
        m_old = m_ref[:, at]
        m_new = jnp.maximum(m_old, jnp.max(s, 0, keepdims=True))
        shrink = jnp.exp2(m_old - m_new)
        p = jnp.exp2(s - m_new)
        l_ref[:, at] = l_ref[:, at] * shrink + jnp.sum(p, 0, keepdims=True)
        m_ref[:, at] = m_new
        pv = jnp.dot(v_t, p.astype(jnp.bfloat16), preferred_element_type=jnp.float32)
        acc_ref[:, at] = acc_ref[:, at] * shrink + pv
        s = following

    @pl.when(step == pl.num_programs(0) - 1)
    def _():
        for h in range(heads):
            at = slice(h * tokens, (h + 1) * tokens)
            out = acc_ref[:, at] / l_ref[:, at]
            o_ref[:, h * width : (h + 1) * width] = out.T.astype(jnp.bfloat16)


def attention(q_t, keys_values, tokens, width):
    length = keys_values.shape[0]
    rows = q_t.shape[1]
    block = min(KEY_BLOCK, length)
    heads = rows // tokens
    return pl.pallas_call(
        attention_kernel,
        grid=(length // block,),
        in_specs=[
            pl.BlockSpec(q_t.shape, lambda i: (0, 0)),
            pl.BlockSpec((block, width), lambda i: (i, 0)),
            pl.BlockSpec((block, width), lambda i: (i, 1)),
        ],
        out_specs=pl.BlockSpec((tokens, heads * width), lambda i: (0, 0)),
        out_shape=jax.ShapeDtypeStruct((tokens, heads * width), jnp.bfloat16),
        scratch_shapes=[
            pltpu.VMEM((1, rows), jnp.float32),
            pltpu.VMEM((1, rows), jnp.float32),
            pltpu.VMEM((width, rows), jnp.float32),
        ],
        compiler_params=pltpu.CompilerParams(vmem_limit_bytes=VMEM_LIMIT),
        cost_estimate=pl.CostEstimate(
            flops=4 * rows * length * width,
            bytes_accessed=length * width * 4,
            transcendentals=rows * length,
        ),
        name="attention",
    )(q_t, keys_values, keys_values)


def half_rows(rows, columns):
    row = lax.broadcasted_iota(jnp.int32, (rows, columns), 0)
    return ((row % 8) < 4).astype(jnp.float32)


def widened(block, left):
    value = block.astype(jnp.float32)
    first = value * left
    return jnp.concatenate([first, value - first], 1).astype(jnp.bfloat16)


def halves_added(value):
    rows, columns = value.shape
    parts = value.reshape(rows // 8, 8, columns)
    return (parts + pltpu.roll(parts, 4, 1)).reshape(rows, columns)


def moe_kernel(
    out_ref,
    wg_ref,
    wu_ref,
    wd_ref,
    ret_ref,
    x_ref,
    h_ref,
    y_ref,
    go_send,
    go_recv,
    ring_send,
    ring_recv,
    pass_send,
    pass_recv,
    hid_send,
    hid_recv,
    back_send,
    back_recv,
):
    sp = lax.axis_index("sp")
    lane = lax.axis_index("tp")
    core = lax.rem(sp, 2)
    x_at = lax.rem(sp // 2, X_SIZE)
    z_at = sp // (2 * X_SIZE)
    right = lax.rem(lane + 1, LANES)
    left = lax.rem(lane + LANES - 1, LANES)
    far = lax.rem(lane + 2, LANES)
    wide = wd_ref.shape[1]
    half = wide // 2
    deep = wd_ref.shape[0] // LANES
    peers = X_SIZE * 2
    group = 8 * peers
    count = Z_SIZE

    def z_offset(p):
        return jnp.where(lax.rem(p, 2) == 1, (p + 1) // 2, lax.rem(Z_SIZE - p // 2, Z_SIZE))

    def peer(index, sign):
        p = index // peers
        dx = lax.rem(index, peers) // 2
        dc = lax.rem(index, 2)
        z = lax.rem(z_at + sign * z_offset(p) + Z_SIZE, Z_SIZE)
        x = lax.rem(x_at + sign * dx + X_SIZE, X_SIZE)
        c = lax.rem(core + dc, 2)
        return (z * X_SIZE + x) * 2 + c

    def rows_of(index):
        return pl.ds(pl.multiple_of(index * 8, 8), 8)

    def group_rows(p):
        return pl.ds(pl.multiple_of(p * group, group), group)

    barrier = pltpu.get_barrier_semaphore()

    def greet(index, _):
        pl.semaphore_signal(
            barrier, inc=1, device_id={"sp": peer(index, 1), "tp": lane}, device_id_type=MESH
        )
        return 0

    lax.fori_loop(1, count * peers, greet, 0)
    for other in (left, right, far):
        pl.semaphore_signal(
            barrier, inc=1, device_id={"sp": sp, "tp": other}, device_id_type=MESH
        )
    pl.semaphore_wait(barrier, count * peers - 1 + LANES - 1)

    def go(index):
        return pltpu.make_async_remote_copy(
            src_ref=out_ref.at[rows_of(index)],
            dst_ref=x_ref.at[lane, rows_of(index)],
            send_sem=go_send.at[index],
            recv_sem=go_recv.at[index],
            device_id={"sp": peer(index, 1), "tp": lane},
            device_id_type=MESH,
        )

    def back(index):
        return pltpu.make_async_remote_copy(
            src_ref=y_ref.at[rows_of(index)],
            dst_ref=ret_ref.at[rows_of(index)],
            send_sem=back_send.at[index],
            recv_sem=back_recv.at[index],
            device_id={"sp": peer(index, -1), "tp": lane},
            device_id_type=MESH,
        )

    def ring(p, way):
        return pltpu.make_async_remote_copy(
            src_ref=x_ref.at[lane, group_rows(p)],
            dst_ref=x_ref.at[lane, group_rows(p)],
            send_sem=ring_send.at[p, way],
            recv_sem=ring_recv.at[p, way],
            device_id={"sp": sp, "tp": right if way == 0 else left},
            device_id_type=MESH,
        )

    def passed(p, way):
        owner = left if way == 0 else right
        rows = pl.ds(pl.multiple_of(p * group + way * (group // 2), group // 2), group // 2)
        return pltpu.make_async_remote_copy(
            src_ref=x_ref.at[owner, rows],
            dst_ref=x_ref.at[owner, rows],
            send_sem=pass_send.at[p, way],
            recv_sem=pass_recv.at[p, way],
            device_id={"sp": sp, "tp": right if way == 0 else left},
            device_id_type=MESH,
        )

    def hid(p, way):
        return pltpu.make_async_remote_copy(
            src_ref=h_ref.at[lane, group_rows(p)],
            dst_ref=h_ref.at[lane, group_rows(p)],
            send_sem=hid_send.at[p, way],
            recv_sem=hid_recv.at[p, way],
            device_id={"sp": sp, "tp": (right, left, far)[way]},
            device_id_type=MESH,
        )

    own_in = pltpu.make_async_copy(
        out_ref.at[pl.ds(0, 8)], x_ref.at[lane, pl.ds(0, 8)], go_recv.at[0]
    )
    own_out = pltpu.make_async_copy(y_ref.at[pl.ds(0, 8)], ret_ref.at[pl.ds(0, 8)], back_recv.at[0])
    own_in.start()

    def send_one(index, _):
        go(index).start()
        return 0

    lax.fori_loop(1, count * peers, send_one, 0)

    def hidden_of(p):
        rows = group_rows(p)
        left_half = half_rows(group, half)
        gate = None
        up = None
        for j in range(LANES):
            lhs = jnp.concatenate(
                [x_ref[j, rows, :wide], widened(x_ref[j, rows, wide:], left_half)], 0
            )
            g = jnp.dot(
                lhs, wg_ref[j * wide : (j + 1) * wide, :], preferred_element_type=jnp.float32
            )
            u = jnp.dot(
                lhs, wu_ref[j * wide : (j + 1) * wide, :], preferred_element_type=jnp.float32
            )
            gate = g if gate is None else gate + g
            up = u if up is None else up + u
        gate = jnp.concatenate([gate[:group], halves_added(gate[group:])], 0)
        up = jnp.concatenate([up[:group], halves_added(up[group:])], 0)
        hidden = gate / (1.0 + jnp.exp(-gate)) * up
        low = hidden[group:, : deep // 2]
        high = hidden[group:, deep // 2 :]
        narrow = jnp.where(half_rows(group, deep // 2) > 0.0, low, high)
        h_ref[lane, rows, :deep] = hidden[:group].astype(jnp.bfloat16)
        h_ref[lane, rows, deep:] = narrow.astype(jnp.bfloat16)

    def output_of(p):
        rows = group_rows(p)
        left_half = half_rows(group, deep // 2)
        total_a = None
        total_b = None
        for j in range(LANES):
            lhs = jnp.concatenate(
                [h_ref[j, rows, :deep], widened(h_ref[j, rows, deep:], left_half)], 0
            )
            z = jnp.dot(
                lhs, wd_ref[j * deep : (j + 1) * deep, :], preferred_element_type=jnp.float32
            )
            a = z[:group].astype(jnp.bfloat16).astype(jnp.float32)
            b = halves_added(z[group:]).astype(jnp.bfloat16).astype(jnp.float32)
            total_a = a if total_a is None else total_a + a
            total_b = b if total_b is None else total_b + b
        narrow = jnp.where(half_rows(group, half) > 0.0, total_b[:, :half], total_b[:, half:])
        y_ref[rows, :wide] = total_a.astype(jnp.bfloat16)
        y_ref[rows, wide:] = narrow.astype(jnp.bfloat16)

    def step(t, _):
        @pl.when(t < count)
        def _():
            @pl.when(t == 0)
            def _():
                own_in.wait()

            def arrived(i, _):
                index = t * peers + i

                @pl.when(index > 0)
                def _():
                    go(index).wait_recv()

                return 0

            lax.fori_loop(0, peers, arrived, 0)
            ring(t, 0).start()
            ring(t, 1).start()

        @pl.when((t >= 1) & (t < count + 1))
        def _():
            ring(t - 1, 0).wait_recv()
            passed(t - 1, 0).start()
            ring(t - 1, 1).wait_recv()
            passed(t - 1, 1).start()

        @pl.when((t >= 2) & (t < count + 2))
        def _():
            passed(t - 2, 0).wait_recv()
            passed(t - 2, 1).wait_recv()
            hidden_of(t - 2)
            for way in range(LANES - 1):
                hid(t - 2, way).start()

        @pl.when(t >= 3)
        def _():
            for way in range(LANES - 1):
                hid(t - 3, way).wait_recv()
            output_of(t - 3)

            @pl.when(t == 3)
            def _():
                own_out.start()

            def send_back(i, _):
                index = (t - 3) * peers + i

                @pl.when(index > 0)
                def _():
                    back(index).start()

                return 0

            lax.fori_loop(0, peers, send_back, 0)

        return 0

    lax.fori_loop(0, count + 3, step, 0)
    own_out.wait()

    def finish(index, _):
        go(index).wait_send()
        back(index).wait_send()
        back(index).wait_recv()
        return 0

    lax.fori_loop(1, count * peers, finish, 0)

    def finish_group(p, _):
        for way in range(2):
            ring(p, way).wait_send()
            passed(p, way).wait_send()
        for way in range(LANES - 1):
            hid(p, way).wait_send()
        return 0

    lax.fori_loop(0, count, finish_group, 0)


def moe_layer(outgoing, w_gate, w_up, w_down):
    rows, columns = outgoing.shape
    hidden = w_gate.shape[1]
    blocks = rows // 8
    vmem = pl.BlockSpec(memory_space=pltpu.VMEM)
    dma = pltpu.SemaphoreType.DMA
    return pl.pallas_call(
        moe_kernel,
        in_specs=[vmem] * 4,
        out_specs=vmem,
        out_shape=jax.ShapeDtypeStruct((rows, columns), jnp.bfloat16),
        scratch_shapes=[
            pltpu.VMEM((LANES, rows, columns), jnp.bfloat16),
            pltpu.VMEM((LANES, rows, hidden * 3 // 2), jnp.bfloat16),
            pltpu.VMEM((rows, columns), jnp.bfloat16),
            dma((blocks,)),
            dma((blocks,)),
            dma((Z_SIZE, 2)),
            dma((Z_SIZE, 2)),
            dma((Z_SIZE, 2)),
            dma((Z_SIZE, 2)),
            dma((Z_SIZE, LANES - 1)),
            dma((Z_SIZE, LANES - 1)),
            dma((blocks,)),
            dma((blocks,)),
        ],
        compiler_params=pltpu.CompilerParams(
            vmem_limit_bytes=VMEM_LIMIT, collective_id=1, has_side_effects=True
        ),
        cost_estimate=pl.CostEstimate(
            flops=12 * LANES * rows * 1024 * hidden,
            bytes_accessed=200_000_000,
            transcendentals=0,
        ),
        name="experts",
    )(outgoing, w_gate, w_up, w_down)


def split_layer_norm(z, gain):
    local = z.shape[-1]
    mean = jnp.mean(z, -1)
    centre = z - mean[:, None]
    m2 = jnp.sum(centre * centre, -1)
    both = lax.all_gather(jnp.stack([mean, m2]), "tp", axis=0, tiled=False)
    means, m2s = both[:, 0], both[:, 1]
    full_mean = jnp.mean(means, 0)
    away = means - full_mean[None]
    spread = (jnp.sum(m2s, 0) + local * jnp.sum(away * away, 0)) / (local * both.shape[0])
    return (z - full_mean[:, None]) * lax.rsqrt(spread + 1e-06)[:, None] * gain


def per_device(
    resid,
    queries,
    keys,
    values,
    q_gain,
    key_norm_gain,
    out_weight,
    norm1_gain,
    norm2_gain,
    expert_ids,
    group_weight,
    expert_weight,
    gate_proj,
    up_proj,
    down_proj,
):
    tokens = queries.shape[0]
    width = q_gain.shape[0]
    heads = queries.shape[1] // width
    lanes = lax.axis_size("tp")
    sp_count = lax.axis_size("sp")
    lane = lax.axis_index("tp")
    own = tokens // lanes
    model_width = resid.shape[1]
    part = model_width // lanes

    positions = lax.axis_index("sp") * tokens + jnp.arange(tokens, dtype=jnp.int32)
    rotated_keys = apply_rotary_heads(keys.reshape(tokens, 1, width), key_norm_gain, positions)
    both = jnp.concatenate([rotated_keys.reshape(tokens, width), values], 1)
    keys_values = lax.all_gather(both, "sp", axis=0, tiled=True)

    out_slice = lax.all_to_all(out_weight, "tp", split_axis=1, concat_axis=0, tiled=True)
    down_slice = lax.all_to_all(down_proj[0], "tp", split_axis=1, concat_axis=0, tiled=True)
    resid_slice = lax.all_to_all(resid, "tp", split_axis=1, concat_axis=0, tiled=True)
    ids = lax.all_gather(expert_ids, "tp", axis=0, tiled=True)
    gates_own = (
        group_weight[:, None] * expert_weight / jnp.sum(expert_weight, -1, keepdims=True)
    )
    gates = lax.all_gather(gates_own, "tp", axis=0, tiled=True)

    q_rot = apply_rotary_heads(queries.reshape(tokens, heads, width), q_gain, positions)
    factor = np.float32(np.log2(np.e) * width**-0.5)
    scaled = q_rot.astype(jnp.float32) * factor
    coarse = lax.reduce_precision(scaled, 8, 7)
    fine = (scaled - coarse).astype(jnp.bfloat16)
    pair = jnp.concatenate([coarse.astype(jnp.bfloat16), fine], -1)
    q_t = pair.transpose(2, 1, 0).reshape(2 * width, heads * tokens)
    attn = attention(q_t, keys_values, tokens, width)
    attn = lax.all_gather(attn, "tp", axis=1, tiled=True)

    proj = jnp.dot(attn, out_slice, preferred_element_type=jnp.float32)
    proj = lax.reduce_precision(proj, 8, 7)
    summed = deep_alpha * resid_slice.astype(jnp.float32) + proj
    gain_one = lax.dynamic_slice_in_dim(norm1_gain, lane * part, part)
    gain_two = lax.dynamic_slice_in_dim(norm2_gain, lane * part, part)
    x_one = split_layer_norm(summed, gain_one).astype(jnp.bfloat16)

    top = ids.shape[1]
    half = part // 2
    blocks = ids.reshape(lanes, own * top)
    one_hot = (blocks[:, :, None] == jnp.arange(sp_count, dtype=jnp.int32)).astype(jnp.int32)
    earlier = jnp.cumsum(one_hot, 1) - one_hot
    rank = jnp.sum(earlier * one_hot, 2)
    sp = lax.axis_index("sp")
    dz = (blocks // (2 * X_SIZE) - sp // (2 * X_SIZE)) % Z_SIZE
    dx = (blocks // 2 - sp // 2) % X_SIZE
    dc = (blocks - sp) % 2
    near = jnp.where(dz == 0, 0, jnp.where(dz <= Z_SIZE // 2, 2 * dz - 1, 2 * (Z_SIZE - dz)))
    target = (near * X_SIZE + dx) * 2 + dc
    place = jnp.arange(lanes, dtype=jnp.int32)[:, None] * CAP + rank
    row_a = jnp.where(place < 8, target * 8 + place, -1).reshape(tokens, top)
    row_b = jnp.where(place < 8, -1, target * 8 + place - 8).reshape(tokens, top)
    rows = jnp.arange(sp_count * 8, dtype=jnp.int32)
    picks = (row_a[:, :, None] == rows, row_b[:, :, None] == rows, row_b[:, :, None] + 4 == rows)
    picks = (picks[0], picks[1] & (row_b[:, :, None] >= 0), picks[2] & (row_b[:, :, None] >= 0))

    def placed(pick, source):
        return lax.dot_general(
            jnp.any(pick, 1).astype(jnp.bfloat16),
            source,
            (((0,), (0,)), ((), ())),
            preferred_element_type=jnp.float32,
        )

    outgoing = jnp.concatenate(
        [
            placed(picks[0], x_one),
            placed(picks[1], x_one[:, :half]) + placed(picks[2], x_one[:, half:]),
        ],
        1,
    ).astype(jnp.bfloat16)
    returned = moe_layer(outgoing, gate_proj[0], up_proj[0], down_slice)

    def weighted(pick, source):
        weights = jnp.sum(jnp.where(pick, gates[:, :, None], 0.0), 1)
        total = None
        for _ in range(3):
            term = lax.reduce_precision(weights, 8, 7)
            weights = weights - term
            piece = jnp.dot(
                term.astype(jnp.bfloat16), source, preferred_element_type=jnp.float32
            )
            total = piece if total is None else total + piece
        return total

    moe = weighted(picks[0], returned[:, :part]) + jnp.concatenate(
        [weighted(picks[1], returned[:, part:]), weighted(picks[2], returned[:, part:])], 1
    )
    final = deep_alpha * x_one.astype(jnp.float32) + moe
    mixed = split_layer_norm(final, gain_two).astype(jnp.bfloat16)
    return lax.all_to_all(mixed, "tp", split_axis=0, concat_axis=1, tiled=True)


def solution(mesh):
    in_specs = (
        P(("sp", "tp"), None),
        P("sp", "tp"),
        P("sp", "tp"),
        P("sp", "tp"),
        P(),
        P(),
        P("tp", None),
        P(),
        P(),
        P(("sp", "tp"), None),
        P(("sp", "tp")),
        P(("sp", "tp"), None),
        P("sp", None, "tp"),
        P("sp", None, "tp"),
        P("sp", "tp", None),
    )
    out_specs = P(("sp", "tp"), None)
    return jax.shard_map(
        per_device, mesh=mesh, in_specs=in_specs, out_specs=out_specs, check_vma=False
    )
```

```python
import jax
import jax.numpy as jnp
import numpy as np
from jax import lax
from jax.experimental import pallas as pl
from jax.experimental.pallas import tpu as pltpu
from jax.sharding import PartitionSpec as P

GRID_W = 64
CAP = 3
QUERY_TILE = 512

deep_alpha = 2.0**0.5
rope_theta = 10000.0
VMEM_LIMIT = 60 * 1024 * 1024
MESH = pl.DeviceIdType.MESH
Z_SIZE = 8
X_SIZE = 4
LANES = 4


def apply_rotary_heads(block, gain, grid_positions):
    values32 = block.astype(jnp.float32)
    normed = values32 * lax.rsqrt(jnp.mean(values32 * values32, -1, keepdims=True) + 1e-06) * gain
    half = normed.shape[-1] // 2
    inv_freq = rope_theta ** (-jnp.arange(0, half, 2, dtype=jnp.float32) / half)
    grid_row = (grid_positions // GRID_W).astype(jnp.float32)
    grid_col = (grid_positions % GRID_W).astype(jnp.float32)
    angle = jnp.concatenate([grid_row[:, None] * inv_freq, grid_col[:, None] * inv_freq], -1)[
        :, None, :
    ]
    cosine = jnp.cos(angle)
    sine = jnp.sin(angle)
    first = normed[..., :half]
    second = normed[..., half:]
    turned = jnp.concatenate([first * cosine - second * sine, first * sine + second * cosine], -1)
    return turned.astype(jnp.bfloat16)


def front_kernel(
    qt_ref,
    own_ref,
    w_ref,
    wd_ref,
    resid_ref,
    info_ref,
    gain_ref,
    x_ref,
    down_ref,
    table_ref,
    kv_ref,
    m_ref,
    l_ref,
    acc_ref,
    attn_ref,
    out_ref,
    res_ref,
    stat_ref,
    tx,
    rx_full,
    rx_half,
    rx_core,
    load_sem,
    w_send,
    w_recv,
    w_pair_send,
    w_pair_recv,
    d_send,
    d_recv,
    r_send,
    r_recv,
    i_send,
    i_recv,
    a_send,
    a_recv,
    s_send,
    s_recv,
):
    sp = lax.axis_index("sp")
    lane = lax.axis_index("tp")
    core = lax.rem(sp, 2)
    x_at = lax.rem(sp // 2, X_SIZE)
    z_at = sp // (2 * X_SIZE)
    partner = sp + 1 - 2 * core
    block = own_ref.shape[0]
    width = own_ref.shape[1] // 2
    rows = qt_ref.shape[1]
    heads = rows // block
    wide = x_ref.shape[1]
    lane_rows = res_ref.shape[1]
    depth = out_ref.shape[1]
    lanes_of = [lax.rem(lane + 1, LANES), lax.rem(lane + LANES - 1, LANES), lax.rem(lane + 2, LANES)]
    froms = [lanes_of[1], lanes_of[0], lanes_of[2]]

    def sp_of(z, x, c):
        return (lax.rem(z + 2 * Z_SIZE, Z_SIZE) * X_SIZE + lax.rem(x + 2 * X_SIZE, X_SIZE)) * 2 + c

    ways = (
        sp_of(z_at + 1, x_at, core),
        sp_of(z_at - 1, x_at, core),
        sp_of(z_at, x_at + 1, core),
        sp_of(z_at, x_at - 1, core),
        partner,
    )
    barrier = pltpu.get_barrier_semaphore()
    for way in range(5):
        pl.semaphore_signal(
            barrier, inc=1, device_id={"sp": ways[way], "tp": lane}, device_id_type=MESH
        )
    for other in lanes_of:
        pl.semaphore_signal(
            barrier, inc=1, device_id={"sp": sp, "tp": other}, device_id_type=MESH
        )

    own_copy = pltpu.make_async_copy(own_ref, kv_ref.at[core, z_at, x_at], load_sem.at[0])
    w_copy = pltpu.make_async_copy(
        w_ref.at[:, pl.ds(pl.multiple_of(lane * wide, wide), wide)], out_ref.at[lane], load_sem.at[1]
    )
    d_copy = pltpu.make_async_copy(
        wd_ref.at[:, pl.ds(pl.multiple_of(lane * wide, wide), wide)], down_ref.at[lane], load_sem.at[2]
    )
    r_copy = pltpu.make_async_copy(
        resid_ref.at[:, pl.ds(pl.multiple_of(lane * wide, wide), wide)], res_ref.at[lane], load_sem.at[3]
    )
    i_copy = pltpu.make_async_copy(info_ref, table_ref.at[lane], load_sem.at[4])
    own_copy.start()

    def to_lane(src, dst, send, recv, way):
        return pltpu.make_async_remote_copy(
            src_ref=src,
            dst_ref=dst,
            send_sem=send.at[way],
            recv_sem=recv.at[way],
            device_id={"sp": sp, "tp": lanes_of[way]},
            device_id_type=MESH,
        )

    def columns(way):
        return pl.ds(pl.multiple_of(lanes_of[way] * wide, wide), wide)

    part_rows = depth // 2
    half = pl.ds(pl.multiple_of(core * part_rows, part_rows), part_rows)

    def w_go(way):
        return to_lane(w_ref.at[half, columns(way)], out_ref.at[lane, half], w_send, w_recv, way)

    def w_pair(way):
        return pltpu.make_async_remote_copy(
            src_ref=out_ref.at[froms[way], half],
            dst_ref=out_ref.at[froms[way], half],
            send_sem=w_pair_send.at[way],
            recv_sem=w_pair_recv.at[way],
            device_id={"sp": partner, "tp": lane},
            device_id_type=MESH,
        )

    def d_go(way):
        return to_lane(wd_ref.at[:, columns(way)], down_ref.at[lane], d_send, d_recv, way)

    def r_go(way):
        return to_lane(resid_ref.at[:, columns(way)], res_ref.at[lane], r_send, r_recv, way)

    def i_go(way):
        return to_lane(info_ref, table_ref.at[lane], i_send, i_recv, way)

    def a_go(way):
        return to_lane(attn_ref.at[lane], attn_ref.at[lane], a_send, a_recv, way)

    def s_go(way):
        return to_lane(stat_ref.at[lane], stat_ref.at[lane], s_send, s_recv, way)

    def send(cls, zz, xx, way, piece=None):
        if piece is None:
            at = kv_ref.at[cls, zz, xx]
            recv = rx_core.at[zz, xx] if way == 4 else rx_full.at[zz, xx]
        else:
            at = kv_ref.at[cls, zz, xx, pl.ds(piece * (block // 2), block // 2)]
            recv = rx_half.at[zz, xx, piece]
        return pltpu.make_async_remote_copy(
            src_ref=at,
            dst_ref=at,
            send_sem=tx.at[zz, xx, way],
            recv_sem=recv,
            device_id={"sp": ways[way], "tp": lane},
            device_id_type=MESH,
        )

    def wait_block(zz, xx, halves):
        if halves:
            send(core, zz, xx, 0, 0).wait_recv()
            send(core, zz, xx, 0, 1).wait_recv()
        else:
            send(core, zz, xx, 0).wait_recv()

    def z_of(d):
        return lax.rem(z_at + d + Z_SIZE, Z_SIZE)

    x_order = [
        x_at,
        lax.rem(x_at + X_SIZE - 1, X_SIZE),
        lax.rem(x_at + 1, X_SIZE),
        lax.rem(x_at + 2, X_SIZE),
    ]

    def along_x(zz, s, act):
        if s == 0:
            act(send(core, zz, x_order[0], 2))
            act(send(core, zz, x_order[0], 3))
        elif s == 1:
            act(send(core, zz, x_order[1], 2, 0))
        elif s == 2:
            act(send(core, zz, x_order[2], 3, 1))

    def along_z(h, xx, side, act):
        zz = z_of(-h if side == 0 else h)

        @pl.when(h < 3)
        def _():
            act(send(core, zz, xx, side))

        @pl.when(h == 3)
        def _():
            act(send(core, zz, xx, side, side))

    def first(s, act, wait):
        xx = x_order[s]
        if wait and s > 0:
            wait_block(z_at, xx, s == 3)
        along_x(z_at, s, act)

        if s == 0:
            act(send(core, z_at, xx, 0))
            act(send(core, z_at, xx, 1))
        else:

            @pl.when(core == 0)
            def _():
                act(send(core, z_at, xx, 0))
                act(send(core, z_at, xx, 1))

        act(send(core, z_at, xx, 4))

    def later(h, s, act, wait):
        xx = x_order[s]

        @pl.when(h < 4)
        def _():
            for side in range(2):
                zz = z_of(-h if side == 0 else h)

                @pl.when(core == 0)
                def _():
                    if wait:
                        wait_block(zz, xx, False)
                    along_z(h, xx, side, act)

                @pl.when(core == 1)
                def _():
                    if wait:
                        wait_block(zz, xx, s == 3)
                    if s == 0:
                        along_z(h, xx, side, act)
                    along_x(zz, s, act)

                act(send(core, zz, xx, 4))

        @pl.when(h == 4)
        def _():
            zz = z_of(4)
            if wait:
                if s in (0, 3):
                    wait_block(zz, xx, True)
                else:

                    @pl.when(core == 0)
                    def _():
                        wait_block(zz, xx, True)

                    @pl.when(core == 1)
                    def _():
                        wait_block(zz, xx, False)

            @pl.when(core == 1)
            def _():
                along_x(zz, s, act)

            act(send(core, zz, xx, 4))

    def start(copy):
        copy.start()

    def ended(copy):
        copy.wait_send()

    m_ref[...] = jnp.full_like(m_ref, -1e30)
    l_ref[...] = jnp.zeros_like(l_ref)
    acc_ref[...] = jnp.zeros_like(acc_ref)
    own_copy.wait()
    pl.semaphore_wait(barrier, 5 + LANES - 1)
    first(0, start, True)
    for way in range(LANES - 1):
        i_go(way).start()
    for way in range(LANES - 1):
        w_go(way).start()
    for way in range(LANES - 1):
        r_go(way).start()
    for way in range(2):
        d_go(way).start()
    w_copy.start()
    r_copy.start()
    d_copy.start()
    i_copy.start()
    for s in range(1, 4):
        first(s, start, True)

    tile = min(QUERY_TILE, rows)
    keys = X_SIZE * block

    def attend(cls, zz):
        both = kv_ref[cls, zz].reshape(keys, 2 * width)
        k = both[:, :width]
        k_twice = jnp.concatenate([k, k], 1)
        v_t = both[:, width:].T

        def scores(t):
            return jnp.dot(
                k_twice, qt_ref[:, t * tile : (t + 1) * tile], preferred_element_type=jnp.float32
            )

        s = scores(0)
        for t in range(rows // tile):
            following = scores(t + 1) if t + 1 < rows // tile else None
            at = slice(t * tile, (t + 1) * tile)
            m_old = m_ref[:, at]
            m_new = jnp.maximum(m_old, jnp.max(s, 0, keepdims=True))
            shrink = jnp.exp2(m_old - m_new)
            p = jnp.exp2(s - m_new)
            l_ref[:, at] = l_ref[:, at] * shrink + jnp.sum(p, 0, keepdims=True)
            m_ref[:, at] = m_new
            pv = jnp.dot(v_t, p.astype(jnp.bfloat16), preferred_element_type=jnp.float32)
            acc_ref[:, at] = acc_ref[:, at] * shrink + pv
            s = following

    def slot(i, _):
        dist = jnp.where(i < 2, 0, (i - 2) // 4 + 1)
        turn = lax.rem(i + 2, 4)
        ours = jnp.where((dist == 0) | (dist == 4), lax.rem(i, 2) == 0, turn < 2)
        side = jnp.where((dist == 0) | (dist == 4), 1, lax.rem(i, 2))
        zz = z_of(jnp.where(side == 0, -dist, dist))
        cls = jnp.where(ours, core, 1 - core)

        @pl.when(cls != core)
        def _():
            for xx in range(X_SIZE):
                pltpu.make_async_remote_copy(
                    src_ref=kv_ref.at[cls, zz, xx],
                    dst_ref=kv_ref.at[cls, zz, xx],
                    send_sem=tx.at[zz, xx, 4],
                    recv_sem=rx_core.at[zz, xx],
                    device_id={"sp": partner, "tp": lane},
                    device_id_type=MESH,
                ).wait_recv()

        attend(cls, zz)
        for s in range(4):

            @pl.when(((i < 2) & (s // 2 == i)) | ((i >= 2) & (i < 14) & (turn == s)))
            def _(s=s):
                later(dist + 1, s, start, True)

        @pl.when(i == 12)
        def _():
            for way in range(LANES - 1):
                w_go(way).wait_recv()
                w_pair(way).start()

        return 0

    lax.fori_loop(0, 16, slot, 0)

    for h in range(heads):
        at = slice(h * block, (h + 1) * block)
        out = acc_ref[:, at] / l_ref[:, at]
        attn_ref[lane, :, h * width : (h + 1) * width] = out.T.astype(jnp.bfloat16)
    for way in range(LANES - 1):
        a_go(way).start()
    d_go(2).start()
    w_copy.wait()
    for way in range(LANES - 1):
        w_pair(way).wait_recv()
    total = jnp.dot(attn_ref[lane], out_ref[lane], preferred_element_type=jnp.float32)
    for way in range(LANES - 1):
        a_go(way).wait_recv()
        total = total + jnp.dot(
            attn_ref[froms[way]], out_ref[froms[way]], preferred_element_type=jnp.float32
        )
    r_copy.wait()
    for way in range(LANES - 1):
        r_go(way).wait_recv()
    summed = deep_alpha * res_ref[...].reshape(LANES * lane_rows, wide).astype(jnp.float32)
    summed = summed + total.astype(jnp.bfloat16).astype(jnp.float32)
    normed = norm_over_lanes(summed, gain_ref[...], stat_ref, s_go, lane)
    x_ref[...] = normed.astype(jnp.bfloat16)

    i_copy.wait()
    d_copy.wait()
    for way in range(LANES - 1):
        i_go(way).wait_recv()
        d_go(way).wait_recv()
        w_go(way).wait_send()
        w_pair(way).wait_send()
        r_go(way).wait_send()
        i_go(way).wait_send()
        d_go(way).wait_send()
        a_go(way).wait_send()
        s_go(way).wait_send()
    for s in range(4):
        first(s, ended, False)

    def finish(h, _):
        for s in range(4):
            later(h, s, ended, False)
        return 0

    lax.fori_loop(1, 5, finish, 0)


def norm_over_lanes(z, gain, stat_ref, s_go, lane):
    rows, wide = z.shape
    mean = jnp.sum(z, 1, keepdims=True) * (1.0 / wide)
    centre = z - mean
    m2 = jnp.sum(centre * centre, 1, keepdims=True)
    column = lax.broadcasted_iota(jnp.int32, (rows, 128), 1)
    both = jnp.where(column == 0, mean, m2)
    stat_ref[lane] = both.T[:8]
    for way in range(LANES - 1):
        s_go(way).start()
    for way in range(LANES - 1):
        s_go(way).wait_recv()
    means = [stat_ref[j][0:1] for j in range(LANES)]
    m2s = [stat_ref[j][1:2] for j in range(LANES)]
    full = (means[0] + means[1] + means[2] + means[3]) * (1.0 / LANES)
    away = sum((v - full) * (v - full) for v in means)
    spread = (m2s[0] + m2s[1] + m2s[2] + m2s[3] + wide * away) * (1.0 / (wide * LANES))
    scale = lax.rsqrt(spread + 1e-06)
    row = lax.broadcasted_iota(jnp.int32, (128, rows), 0)
    packed = jnp.where(row == 0, full, scale).T
    return (z - packed[:, 0:1]) * packed[:, 1:2] * gain


def front(q_t, keys_values, out_weight, down_proj, resid, info, gain):
    tokens, pair = keys_values.shape
    width = pair // 2
    rows = q_t.shape[1]
    depth, model = out_weight.shape
    wide = model // LANES
    vmem = pl.BlockSpec(memory_space=pltpu.VMEM)
    hbm = pl.BlockSpec(memory_space=pltpu.HBM)
    dma = pltpu.SemaphoreType.DMA
    others = LANES - 1
    return pl.pallas_call(
        front_kernel,
        in_specs=[vmem, vmem, hbm, hbm, hbm, vmem, vmem],
        out_specs=[vmem, vmem, vmem],
        out_shape=[
            jax.ShapeDtypeStruct((tokens, wide), jnp.bfloat16),
            jax.ShapeDtypeStruct((LANES, down_proj.shape[0], wide), jnp.bfloat16),
            jax.ShapeDtypeStruct((LANES, *info.shape), jnp.float32),
        ],
        scratch_shapes=[
            pltpu.VMEM((2, Z_SIZE, X_SIZE, tokens, pair), jnp.bfloat16),
            pltpu.VMEM((1, rows), jnp.float32),
            pltpu.VMEM((1, rows), jnp.float32),
            pltpu.VMEM((width, rows), jnp.float32),
            pltpu.VMEM((LANES, tokens, depth), jnp.bfloat16),
            pltpu.VMEM((LANES, depth, wide), jnp.bfloat16),
            pltpu.VMEM((LANES, resid.shape[0], wide), jnp.bfloat16),
            pltpu.VMEM((LANES, 8, tokens), jnp.float32),
            dma((Z_SIZE, X_SIZE, 5)),
            dma((Z_SIZE, X_SIZE)),
            dma((Z_SIZE, X_SIZE, 2)),
            dma((Z_SIZE, X_SIZE)),
            dma((5,)),
        ]
        + [dma((others,))] * 14,
        compiler_params=pltpu.CompilerParams(
            vmem_limit_bytes=VMEM_LIMIT, collective_id=2, has_side_effects=True
        ),
        cost_estimate=pl.CostEstimate(
            flops=20_000_000_000, bytes_accessed=100_000_000, transcendentals=rows * 16384
        ),
        name="front",
    )(q_t, keys_values, out_weight, down_proj, resid, info, gain)


def half_rows(rows, columns):
    row = lax.broadcasted_iota(jnp.int32, (rows, columns), 0)
    return ((row % 8) < 4).astype(jnp.float32)


def widened(block, left):
    value = block.astype(jnp.float32)
    first = value * left
    return jnp.concatenate([first, value - first], 1).astype(jnp.bfloat16)


def halves_added(value):
    rows, columns = value.shape
    parts = value.reshape(rows // 8, 8, columns)
    return (parts + pltpu.roll(parts, 4, 1)).reshape(rows, columns)


def moe_kernel(
    out_ref,
    wg_ref,
    wu_ref,
    wd_ref,
    ret_ref,
    x_ref,
    h_ref,
    y_ref,
    go_send,
    go_recv,
    ring_send,
    ring_recv,
    pass_send,
    pass_recv,
    hid_send,
    hid_recv,
    back_send,
    back_recv,
):
    sp = lax.axis_index("sp")
    lane = lax.axis_index("tp")
    core = lax.rem(sp, 2)
    x_at = lax.rem(sp // 2, X_SIZE)
    z_at = sp // (2 * X_SIZE)
    right = lax.rem(lane + 1, LANES)
    left = lax.rem(lane + LANES - 1, LANES)
    far = lax.rem(lane + 2, LANES)
    wide = wd_ref.shape[1]
    half = wide // 2
    deep = wd_ref.shape[0] // LANES
    peers = X_SIZE * 2
    group = 8 * peers
    count = Z_SIZE

    def z_offset(p):
        return jnp.where(lax.rem(p, 2) == 1, (p + 1) // 2, lax.rem(Z_SIZE - p // 2, Z_SIZE))

    def peer(index, sign):
        p = index // peers
        dx = lax.rem(index, peers) // 2
        dc = lax.rem(index, 2)
        z = lax.rem(z_at + sign * z_offset(p) + Z_SIZE, Z_SIZE)
        x = lax.rem(x_at + sign * dx + X_SIZE, X_SIZE)
        c = lax.rem(core + dc, 2)
        return (z * X_SIZE + x) * 2 + c

    def rows_of(index):
        return pl.ds(pl.multiple_of(index * 8, 8), 8)

    def group_rows(p):
        return pl.ds(pl.multiple_of(p * group, group), group)

    barrier = pltpu.get_barrier_semaphore()

    def greet(index, _):
        pl.semaphore_signal(
            barrier, inc=1, device_id={"sp": peer(index, 1), "tp": lane}, device_id_type=MESH
        )
        return 0

    lax.fori_loop(1, count * peers, greet, 0)
    for other in (left, right, far):
        pl.semaphore_signal(
            barrier, inc=1, device_id={"sp": sp, "tp": other}, device_id_type=MESH
        )
    pl.semaphore_wait(barrier, count * peers - 1 + LANES - 1)

    def go(index):
        return pltpu.make_async_remote_copy(
            src_ref=out_ref.at[rows_of(index)],
            dst_ref=x_ref.at[lane, rows_of(index)],
            send_sem=go_send.at[index],
            recv_sem=go_recv.at[index],
            device_id={"sp": peer(index, 1), "tp": lane},
            device_id_type=MESH,
        )

    def back(index):
        return pltpu.make_async_remote_copy(
            src_ref=y_ref.at[rows_of(index)],
            dst_ref=ret_ref.at[rows_of(index)],
            send_sem=back_send.at[index],
            recv_sem=back_recv.at[index],
            device_id={"sp": peer(index, -1), "tp": lane},
            device_id_type=MESH,
        )

    def ring(p, way):
        return pltpu.make_async_remote_copy(
            src_ref=x_ref.at[lane, group_rows(p)],
            dst_ref=x_ref.at[lane, group_rows(p)],
            send_sem=ring_send.at[p, way],
            recv_sem=ring_recv.at[p, way],
            device_id={"sp": sp, "tp": right if way == 0 else left},
            device_id_type=MESH,
        )

    def passed(p, way):
        owner = left if way == 0 else right
        rows = pl.ds(pl.multiple_of(p * group + way * (group // 2), group // 2), group // 2)
        return pltpu.make_async_remote_copy(
            src_ref=x_ref.at[owner, rows],
            dst_ref=x_ref.at[owner, rows],
            send_sem=pass_send.at[p, way],
            recv_sem=pass_recv.at[p, way],
            device_id={"sp": sp, "tp": right if way == 0 else left},
            device_id_type=MESH,
        )

    def hid(p, way):
        return pltpu.make_async_remote_copy(
            src_ref=h_ref.at[lane, group_rows(p)],
            dst_ref=h_ref.at[lane, group_rows(p)],
            send_sem=hid_send.at[p, way],
            recv_sem=hid_recv.at[p, way],
            device_id={"sp": sp, "tp": (right, left, far)[way]},
            device_id_type=MESH,
        )

    own_in = pltpu.make_async_copy(
        out_ref.at[pl.ds(0, 8)], x_ref.at[lane, pl.ds(0, 8)], go_recv.at[0]
    )
    own_out = pltpu.make_async_copy(y_ref.at[pl.ds(0, 8)], ret_ref.at[pl.ds(0, 8)], back_recv.at[0])
    own_in.start()

    def send_one(index, _):
        go(index).start()
        return 0

    lax.fori_loop(1, count * peers, send_one, 0)

    def hidden_of(p):
        rows = group_rows(p)
        left_half = half_rows(group, half)
        gate = None
        up = None
        for j in range(LANES):
            lhs = jnp.concatenate(
                [x_ref[j, rows, :wide], widened(x_ref[j, rows, wide:], left_half)], 0
            )
            g = jnp.dot(
                lhs, wg_ref[j * wide : (j + 1) * wide, :], preferred_element_type=jnp.float32
            )
            u = jnp.dot(
                lhs, wu_ref[j * wide : (j + 1) * wide, :], preferred_element_type=jnp.float32
            )
            gate = g if gate is None else gate + g
            up = u if up is None else up + u
        gate = jnp.concatenate([gate[:group], halves_added(gate[group:])], 0)
        up = jnp.concatenate([up[:group], halves_added(up[group:])], 0)
        hidden = gate / (1.0 + jnp.exp(-gate)) * up
        low = hidden[group:, : deep // 2]
        high = hidden[group:, deep // 2 :]
        narrow = jnp.where(half_rows(group, deep // 2) > 0.0, low, high)
        h_ref[lane, rows, :deep] = hidden[:group].astype(jnp.bfloat16)
        h_ref[lane, rows, deep:] = narrow.astype(jnp.bfloat16)

    def output_of(p):
        rows = group_rows(p)
        left_half = half_rows(group, deep // 2)
        total_a = None
        total_b = None
        for j in range(LANES):
            lhs = jnp.concatenate(
                [h_ref[j, rows, :deep], widened(h_ref[j, rows, deep:], left_half)], 0
            )
            z = jnp.dot(
                lhs, wd_ref[j * deep : (j + 1) * deep, :], preferred_element_type=jnp.float32
            )
            a = z[:group].astype(jnp.bfloat16).astype(jnp.float32)
            b = halves_added(z[group:]).astype(jnp.bfloat16).astype(jnp.float32)
            total_a = a if total_a is None else total_a + a
            total_b = b if total_b is None else total_b + b
        narrow = jnp.where(half_rows(group, half) > 0.0, total_b[:, :half], total_b[:, half:])
        y_ref[rows, :wide] = total_a.astype(jnp.bfloat16)
        y_ref[rows, wide:] = narrow.astype(jnp.bfloat16)

    def step(t, _):
        @pl.when(t < count)
        def _():
            @pl.when(t == 0)
            def _():
                own_in.wait()

            def arrived(i, _):
                index = t * peers + i

                @pl.when(index > 0)
                def _():
                    go(index).wait_recv()

                return 0

            lax.fori_loop(0, peers, arrived, 0)
            ring(t, 0).start()
            ring(t, 1).start()

        @pl.when((t >= 1) & (t < count + 1))
        def _():
            ring(t - 1, 0).wait_recv()
            passed(t - 1, 0).start()
            ring(t - 1, 1).wait_recv()
            passed(t - 1, 1).start()

        @pl.when((t >= 2) & (t < count + 2))
        def _():
            passed(t - 2, 0).wait_recv()
            passed(t - 2, 1).wait_recv()
            hidden_of(t - 2)
            for way in range(LANES - 1):
                hid(t - 2, way).start()

        @pl.when(t >= 3)
        def _():
            for way in range(LANES - 1):
                hid(t - 3, way).wait_recv()
            output_of(t - 3)

            @pl.when(t == 3)
            def _():
                own_out.start()

            def send_back(i, _):
                index = (t - 3) * peers + i

                @pl.when(index > 0)
                def _():
                    back(index).start()

                return 0

            lax.fori_loop(0, peers, send_back, 0)

        return 0

    lax.fori_loop(0, count + 3, step, 0)
    own_out.wait()

    def finish(index, _):
        go(index).wait_send()
        back(index).wait_send()
        back(index).wait_recv()
        return 0

    lax.fori_loop(1, count * peers, finish, 0)

    def finish_group(p, _):
        for way in range(2):
            ring(p, way).wait_send()
            passed(p, way).wait_send()
        for way in range(LANES - 1):
            hid(p, way).wait_send()
        return 0

    lax.fori_loop(0, count, finish_group, 0)


def moe_layer(outgoing, w_gate, w_up, w_down):
    rows, columns = outgoing.shape
    hidden = w_gate.shape[1]
    blocks = rows // 8
    vmem = pl.BlockSpec(memory_space=pltpu.VMEM)
    dma = pltpu.SemaphoreType.DMA
    return pl.pallas_call(
        moe_kernel,
        in_specs=[vmem] * 4,
        out_specs=vmem,
        out_shape=jax.ShapeDtypeStruct((rows, columns), jnp.bfloat16),
        scratch_shapes=[
            pltpu.VMEM((LANES, rows, columns), jnp.bfloat16),
            pltpu.VMEM((LANES, rows, hidden * 3 // 2), jnp.bfloat16),
            pltpu.VMEM((rows, columns), jnp.bfloat16),
            dma((blocks,)),
            dma((blocks,)),
            dma((Z_SIZE, 2)),
            dma((Z_SIZE, 2)),
            dma((Z_SIZE, 2)),
            dma((Z_SIZE, 2)),
            dma((Z_SIZE, LANES - 1)),
            dma((Z_SIZE, LANES - 1)),
            dma((blocks,)),
            dma((blocks,)),
        ],
        compiler_params=pltpu.CompilerParams(
            vmem_limit_bytes=VMEM_LIMIT, collective_id=1, has_side_effects=True
        ),
        cost_estimate=pl.CostEstimate(
            flops=12 * LANES * rows * 1024 * hidden,
            bytes_accessed=200_000_000,
            transcendentals=0,
        ),
        name="experts",
    )(outgoing, w_gate, w_up, w_down)


def split_layer_norm(z, gain):
    local = z.shape[-1]
    mean = jnp.mean(z, -1)
    centre = z - mean[:, None]
    m2 = jnp.sum(centre * centre, -1)
    both = lax.all_gather(jnp.stack([mean, m2]), "tp", axis=0, tiled=False)
    means, m2s = both[:, 0], both[:, 1]
    full_mean = jnp.mean(means, 0)
    away = means - full_mean[None]
    spread = (jnp.sum(m2s, 0) + local * jnp.sum(away * away, 0)) / (local * both.shape[0])
    return (z - full_mean[:, None]) * lax.rsqrt(spread + 1e-06)[:, None] * gain


def per_device(
    resid,
    queries,
    keys,
    values,
    q_gain,
    key_norm_gain,
    out_weight,
    norm1_gain,
    norm2_gain,
    expert_ids,
    group_weight,
    expert_weight,
    gate_proj,
    up_proj,
    down_proj,
):
    tokens = queries.shape[0]
    width = q_gain.shape[0]
    heads = queries.shape[1] // width
    lanes = lax.axis_size("tp")
    sp_count = lax.axis_size("sp")
    lane = lax.axis_index("tp")
    own = tokens // lanes
    model_width = resid.shape[1]
    part = model_width // lanes

    positions = lax.axis_index("sp") * tokens + jnp.arange(tokens, dtype=jnp.int32)
    rotated_keys = apply_rotary_heads(keys.reshape(tokens, 1, width), key_norm_gain, positions)
    both = jnp.concatenate([rotated_keys.reshape(tokens, width), values], 1)
    gates_own = (
        group_weight[:, None] * expert_weight / jnp.sum(expert_weight, -1, keepdims=True)
    )
    top = expert_ids.shape[1]
    info = jnp.zeros((8, own * top), jnp.float32)
    info = info.at[0].set(expert_ids.reshape(-1).astype(jnp.float32))
    info = info.at[1].set(gates_own.reshape(-1))

    q_rot = apply_rotary_heads(queries.reshape(tokens, heads, width), q_gain, positions)
    factor = np.float32(np.log2(np.e) * width**-0.5)
    scaled = q_rot.astype(jnp.float32) * factor
    coarse = lax.reduce_precision(scaled, 8, 7)
    fine = (scaled - coarse).astype(jnp.bfloat16)
    pair = jnp.concatenate([coarse.astype(jnp.bfloat16), fine], -1)
    q_t = pair.transpose(2, 1, 0).reshape(2 * width, heads * tokens)
    gain_one = lax.dynamic_slice_in_dim(norm1_gain, lane * part, part)
    gain_two = lax.dynamic_slice_in_dim(norm2_gain, lane * part, part)
    x_one, down_slice, table = front(
        q_t, both, out_weight, down_proj[0], resid, info, gain_one[None]
    )
    blocks = table[:, 0].astype(jnp.int32)
    gates = table[:, 1].reshape(tokens, top)

    half = part // 2
    one_hot = (blocks[:, :, None] == jnp.arange(sp_count, dtype=jnp.int32)).astype(jnp.int32)
    earlier = jnp.cumsum(one_hot, 1) - one_hot
    rank = jnp.sum(earlier * one_hot, 2)
    sp = lax.axis_index("sp")
    dz = (blocks // (2 * X_SIZE) - sp // (2 * X_SIZE)) % Z_SIZE
    dx = (blocks // 2 - sp // 2) % X_SIZE
    dc = (blocks - sp) % 2
    near = jnp.where(dz == 0, 0, jnp.where(dz <= Z_SIZE // 2, 2 * dz - 1, 2 * (Z_SIZE - dz)))
    target = (near * X_SIZE + dx) * 2 + dc
    place = jnp.arange(lanes, dtype=jnp.int32)[:, None] * CAP + rank
    row_a = jnp.where(place < 8, target * 8 + place, -1).reshape(tokens, top)
    row_b = jnp.where(place < 8, -1, target * 8 + place - 8).reshape(tokens, top)
    rows = jnp.arange(sp_count * 8, dtype=jnp.int32)
    picks = (row_a[:, :, None] == rows, row_b[:, :, None] == rows, row_b[:, :, None] + 4 == rows)
    picks = (picks[0], picks[1] & (row_b[:, :, None] >= 0), picks[2] & (row_b[:, :, None] >= 0))

    def placed(pick, source):
        return lax.dot_general(
            jnp.any(pick, 1).astype(jnp.bfloat16),
            source,
            (((0,), (0,)), ((), ())),
            preferred_element_type=jnp.float32,
        )

    outgoing = jnp.concatenate(
        [
            placed(picks[0], x_one),
            placed(picks[1], x_one[:, :half]) + placed(picks[2], x_one[:, half:]),
        ],
        1,
    ).astype(jnp.bfloat16)
    returned = moe_layer(
        outgoing, gate_proj[0], up_proj[0], down_slice.reshape(-1, part)
    )

    def weighted(pick, source):
        weights = jnp.sum(jnp.where(pick, gates[:, :, None], 0.0), 1)
        total = None
        for _ in range(3):
            term = lax.reduce_precision(weights, 8, 7)
            weights = weights - term
            piece = jnp.dot(
                term.astype(jnp.bfloat16), source, preferred_element_type=jnp.float32
            )
            total = piece if total is None else total + piece
        return total

    moe = weighted(picks[0], returned[:, :part]) + jnp.concatenate(
        [weighted(picks[1], returned[:, part:]), weighted(picks[2], returned[:, part:])], 1
    )
    final = deep_alpha * x_one.astype(jnp.float32) + moe
    mixed = split_layer_norm(final, gain_two).astype(jnp.bfloat16)
    return lax.all_to_all(mixed, "tp", split_axis=0, concat_axis=1, tiled=True)


def solution(mesh):
    in_specs = (
        P(("sp", "tp"), None),
        P("sp", "tp"),
        P("sp", "tp"),
        P("sp", "tp"),
        P(),
        P(),
        P("tp", None),
        P(),
        P(),
        P(("sp", "tp"), None),
        P(("sp", "tp")),
        P(("sp", "tp"), None),
        P("sp", None, "tp"),
        P("sp", None, "tp"),
        P("sp", "tp", None),
    )
    out_specs = P(("sp", "tp"), None)
    return jax.shard_map(
        per_device, mesh=mesh, in_specs=in_specs, out_specs=out_specs, check_vma=False
    )
```

```python
import jax
import jax.numpy as jnp
import numpy as np
from jax import lax
from jax.experimental import pallas as pl
from jax.experimental.pallas import tpu as pltpu
from jax.sharding import PartitionSpec as P

GRID_W = 64
CAP = 3
QUERY_TILE = 512

deep_alpha = 2.0**0.5
rope_theta = 10000.0
VMEM_LIMIT = 60 * 1024 * 1024
MESH = pl.DeviceIdType.MESH
Z_SIZE = 8
X_SIZE = 4
LANES = 4


def apply_rotary_heads(block, gain, grid_positions):
    values32 = block.astype(jnp.float32)
    normed = values32 * lax.rsqrt(jnp.mean(values32 * values32, -1, keepdims=True) + 1e-06) * gain
    half = normed.shape[-1] // 2
    inv_freq = rope_theta ** (-jnp.arange(0, half, 2, dtype=jnp.float32) / half)
    grid_row = (grid_positions // GRID_W).astype(jnp.float32)
    grid_col = (grid_positions % GRID_W).astype(jnp.float32)
    angle = jnp.concatenate([grid_row[:, None] * inv_freq, grid_col[:, None] * inv_freq], -1)[
        :, None, :
    ]
    cosine = jnp.cos(angle)
    sine = jnp.sin(angle)
    first = normed[..., :half]
    second = normed[..., half:]
    turned = jnp.concatenate([first * cosine - second * sine, first * sine + second * cosine], -1)
    return turned.astype(jnp.bfloat16)


def front_kernel(
    qt_ref,
    own_ref,
    w_ref,
    wd_ref,
    resid_ref,
    info_ref,
    gain_ref,
    x_ref,
    down_ref,
    table_ref,
    kv_ref,
    m_ref,
    l_ref,
    acc_ref,
    attn_ref,
    out_ref,
    res_ref,
    stat_ref,
    tx,
    rx_full,
    rx_half,
    rx_core,
    load_sem,
    w_send,
    w_recv,
    w_pair_send,
    w_pair_recv,
    d_send,
    d_recv,
    r_send,
    r_recv,
    i_send,
    i_recv,
    a_send,
    a_recv,
    s_send,
    s_recv,
):
    sp = lax.axis_index("sp")
    lane = lax.axis_index("tp")
    core = lax.rem(sp, 2)
    x_at = lax.rem(sp // 2, X_SIZE)
    z_at = sp // (2 * X_SIZE)
    partner = sp + 1 - 2 * core
    block = own_ref.shape[0]
    width = own_ref.shape[1] // 2
    rows = qt_ref.shape[1]
    heads = rows // block
    wide = x_ref.shape[1]
    lane_rows = res_ref.shape[1]
    depth = out_ref.shape[1]
    lanes_of = [lax.rem(lane + 1, LANES), lax.rem(lane + LANES - 1, LANES), lax.rem(lane + 2, LANES)]
    froms = [lanes_of[1], lanes_of[0], lanes_of[2]]

    def sp_of(z, x, c):
        return (lax.rem(z + 2 * Z_SIZE, Z_SIZE) * X_SIZE + lax.rem(x + 2 * X_SIZE, X_SIZE)) * 2 + c

    ways = (
        sp_of(z_at + 1, x_at, core),
        sp_of(z_at - 1, x_at, core),
        sp_of(z_at, x_at + 1, core),
        sp_of(z_at, x_at - 1, core),
        partner,
    )
    barrier = pltpu.get_barrier_semaphore()
    for way in range(5):
        pl.semaphore_signal(
            barrier, inc=1, device_id={"sp": ways[way], "tp": lane}, device_id_type=MESH
        )
    for other in lanes_of:
        pl.semaphore_signal(
            barrier, inc=1, device_id={"sp": sp, "tp": other}, device_id_type=MESH
        )

    own_copy = pltpu.make_async_copy(own_ref, kv_ref.at[core, z_at, x_at], load_sem.at[0])
    w_copy = pltpu.make_async_copy(
        w_ref.at[:, pl.ds(pl.multiple_of(lane * wide, wide), wide)], out_ref.at[lane], load_sem.at[1]
    )
    d_copy = pltpu.make_async_copy(
        wd_ref.at[:, pl.ds(pl.multiple_of(lane * wide, wide), wide)], down_ref.at[lane], load_sem.at[2]
    )
    r_copy = pltpu.make_async_copy(
        resid_ref.at[:, pl.ds(pl.multiple_of(lane * wide, wide), wide)], res_ref.at[lane], load_sem.at[3]
    )
    i_copy = pltpu.make_async_copy(info_ref, table_ref.at[lane], load_sem.at[4])
    own_copy.start()

    def to_lane(src, dst, send, recv, way):
        return pltpu.make_async_remote_copy(
            src_ref=src,
            dst_ref=dst,
            send_sem=send.at[way],
            recv_sem=recv.at[way],
            device_id={"sp": sp, "tp": lanes_of[way]},
            device_id_type=MESH,
        )

    def columns(way):
        return pl.ds(pl.multiple_of(lanes_of[way] * wide, wide), wide)

    part_rows = depth // 2
    half = pl.ds(pl.multiple_of(core * part_rows, part_rows), part_rows)

    def w_go(way):
        return to_lane(w_ref.at[half, columns(way)], out_ref.at[lane, half], w_send, w_recv, way)

    def w_pair(way):
        return pltpu.make_async_remote_copy(
            src_ref=out_ref.at[froms[way], half],
            dst_ref=out_ref.at[froms[way], half],
            send_sem=w_pair_send.at[way],
            recv_sem=w_pair_recv.at[way],
            device_id={"sp": partner, "tp": lane},
            device_id_type=MESH,
        )

    def d_go(way):
        return to_lane(wd_ref.at[:, columns(way)], down_ref.at[lane], d_send, d_recv, way)

    def r_go(way):
        return to_lane(resid_ref.at[:, columns(way)], res_ref.at[lane], r_send, r_recv, way)

    def i_go(way):
        return to_lane(info_ref, table_ref.at[lane], i_send, i_recv, way)

    def a_go(way):
        return to_lane(attn_ref.at[lane], attn_ref.at[lane], a_send, a_recv, way)

    def s_go(way):
        return to_lane(stat_ref.at[lane], stat_ref.at[lane], s_send, s_recv, way)

    def send(cls, zz, xx, way, piece=None):
        if piece is None:
            at = kv_ref.at[cls, zz, xx]
            recv = rx_core.at[zz, xx] if way == 4 else rx_full.at[zz, xx]
        else:
            at = kv_ref.at[cls, zz, xx, pl.ds(piece * (block // 2), block // 2)]
            recv = rx_half.at[zz, xx, piece]
        return pltpu.make_async_remote_copy(
            src_ref=at,
            dst_ref=at,
            send_sem=tx.at[zz, xx, way],
            recv_sem=recv,
            device_id={"sp": ways[way], "tp": lane},
            device_id_type=MESH,
        )

    def wait_block(zz, xx, halves):
        if halves:
            send(core, zz, xx, 0, 0).wait_recv()
            send(core, zz, xx, 0, 1).wait_recv()
        else:
            send(core, zz, xx, 0).wait_recv()

    def z_of(d):
        return lax.rem(z_at + d + Z_SIZE, Z_SIZE)

    x_order = [
        x_at,
        lax.rem(x_at + X_SIZE - 1, X_SIZE),
        lax.rem(x_at + 1, X_SIZE),
        lax.rem(x_at + 2, X_SIZE),
    ]

    def along_x(zz, s, act):
        if s == 0:
            act(send(core, zz, x_order[0], 2))
            act(send(core, zz, x_order[0], 3))
        elif s == 1:
            act(send(core, zz, x_order[1], 2, 0))
        elif s == 2:
            act(send(core, zz, x_order[2], 3, 1))

    def along_z(h, xx, side, act):
        zz = z_of(-h if side == 0 else h)

        @pl.when(h < 3)
        def _():
            act(send(core, zz, xx, side))

        @pl.when(h == 3)
        def _():
            act(send(core, zz, xx, side, side))

    def first(s, act, wait):
        xx = x_order[s]
        if wait and s > 0:
            wait_block(z_at, xx, s == 3)
        along_x(z_at, s, act)

        if s == 0:
            act(send(core, z_at, xx, 0))
            act(send(core, z_at, xx, 1))
        else:

            @pl.when(core == 0)
            def _():
                act(send(core, z_at, xx, 0))
                act(send(core, z_at, xx, 1))

        act(send(core, z_at, xx, 4))

    def later(h, s, act, wait):
        xx = x_order[s]

        @pl.when(core == 0)
        def _():
            @pl.when(h < 4)
            def _():
                for side in range(2):
                    zz = z_of(-h if side == 0 else h)
                    if wait:
                        wait_block(zz, xx, False)
                    along_z(h, xx, side, act)
                    act(send(core, zz, xx, 4))

            @pl.when(h == 4)
            def _():
                zz = z_of(4)
                if wait:
                    wait_block(zz, xx, True)
                act(send(core, zz, xx, 4))

        @pl.when(core == 1)
        def _():
            if s == 0:

                @pl.when(h < 4)
                def _():
                    ahead(h + 1, act, wait)
            else:

                @pl.when(h < 4)
                def _():
                    for side in range(2):
                        zz = z_of(-h if side == 0 else h)
                        if wait:
                            wait_block(zz, xx, s == 3)
                        along_x(zz, s, act)
                        act(send(core, zz, xx, 4))

                @pl.when(h == 4)
                def _():
                    zz = z_of(4)
                    if wait:
                        wait_block(zz, xx, s == 3)
                    along_x(zz, s, act)
                    act(send(core, zz, xx, 4))

    def ahead(h, act, wait):
        @pl.when(h < 4)
        def _():
            for side in range(2):
                zz = z_of(-h if side == 0 else h)
                if wait:
                    wait_block(zz, x_at, False)
                along_z(h, x_at, side, act)
                along_x(zz, 0, act)
                act(send(core, zz, x_at, 4))

        @pl.when(h == 4)
        def _():
            zz = z_of(4)
            if wait:
                wait_block(zz, x_at, True)
            along_x(zz, 0, act)
            act(send(core, zz, x_at, 4))

    def start(copy):
        copy.start()

    def ended(copy):
        copy.wait_send()

    m_ref[...] = jnp.full_like(m_ref, -1e30)
    l_ref[...] = jnp.zeros_like(l_ref)
    acc_ref[...] = jnp.zeros_like(acc_ref)
    own_copy.wait()
    pl.semaphore_wait(barrier, 5 + LANES - 1)
    first(0, start, True)
    for way in range(LANES - 1):
        i_go(way).start()
    for way in range(LANES - 1):
        w_go(way).start()
    for way in range(LANES - 1):
        r_go(way).start()
    for way in range(2):
        d_go(way).start()
    w_copy.start()
    r_copy.start()
    d_copy.start()
    i_copy.start()

    @pl.when(core == 1)
    def _():
        ahead(1, start, True)

    for s in range(1, 4):
        first(s, start, True)

    tile = min(QUERY_TILE, rows)
    keys = X_SIZE * block

    def attend(cls, zz):
        both = kv_ref[cls, zz].reshape(keys, 2 * width)
        k = both[:, :width]
        k_twice = jnp.concatenate([k, k], 1)
        v_t = both[:, width:].T

        def scores(t):
            return jnp.dot(
                k_twice, qt_ref[:, t * tile : (t + 1) * tile], preferred_element_type=jnp.float32
            )

        s = scores(0)
        for t in range(rows // tile):
            following = scores(t + 1) if t + 1 < rows // tile else None
            at = slice(t * tile, (t + 1) * tile)
            m_old = m_ref[:, at]
            m_new = jnp.maximum(m_old, jnp.max(s, 0, keepdims=True))
            shrink = jnp.exp2(m_old - m_new)
            p = jnp.exp2(s - m_new)
            l_ref[:, at] = l_ref[:, at] * shrink + jnp.sum(p, 0, keepdims=True)
            m_ref[:, at] = m_new
            pv = jnp.dot(v_t, p.astype(jnp.bfloat16), preferred_element_type=jnp.float32)
            acc_ref[:, at] = acc_ref[:, at] * shrink + pv
            s = following

    def slot(i, _):
        dist = jnp.where(i < 2, 0, (i - 2) // 4 + 1)
        turn = lax.rem(i + 2, 4)
        ours = jnp.where((dist == 0) | (dist == 4), lax.rem(i, 2) == 0, turn < 2)
        side = jnp.where((dist == 0) | (dist == 4), 1, lax.rem(i, 2))
        zz = z_of(jnp.where(side == 0, -dist, dist))
        cls = jnp.where(ours, core, 1 - core)

        @pl.when(cls != core)
        def _():
            for xx in range(X_SIZE):
                pltpu.make_async_remote_copy(
                    src_ref=kv_ref.at[cls, zz, xx],
                    dst_ref=kv_ref.at[cls, zz, xx],
                    send_sem=tx.at[zz, xx, 4],
                    recv_sem=rx_core.at[zz, xx],
                    device_id={"sp": partner, "tp": lane},
                    device_id_type=MESH,
                ).wait_recv()

        attend(cls, zz)
        for s in range(4):

            @pl.when(((i < 2) & (s // 2 == i)) | ((i >= 2) & (i < 14) & (turn == s)))
            def _(s=s):
                later(dist + 1, s, start, True)

        @pl.when(i == 12)
        def _():
            for way in range(LANES - 1):
                w_go(way).wait_recv()
                w_pair(way).start()

        return 0

    lax.fori_loop(0, 16, slot, 0)

    for h in range(heads):
        at = slice(h * block, (h + 1) * block)
        out = acc_ref[:, at] / l_ref[:, at]
        attn_ref[lane, :, h * width : (h + 1) * width] = out.T.astype(jnp.bfloat16)
    for way in range(LANES - 1):
        a_go(way).start()
    d_go(2).start()
    w_copy.wait()
    for way in range(LANES - 1):
        w_pair(way).wait_recv()
    total = jnp.dot(attn_ref[lane], out_ref[lane], preferred_element_type=jnp.float32)
    for way in range(LANES - 1):
        a_go(way).wait_recv()
        total = total + jnp.dot(
            attn_ref[froms[way]], out_ref[froms[way]], preferred_element_type=jnp.float32
        )
    r_copy.wait()
    for way in range(LANES - 1):
        r_go(way).wait_recv()
    summed = deep_alpha * res_ref[...].reshape(LANES * lane_rows, wide).astype(jnp.float32)
    summed = summed + total.astype(jnp.bfloat16).astype(jnp.float32)
    gain = gain_ref[:, pl.ds(pl.multiple_of(lane * wide, wide), wide)]
    normed = norm_over_lanes(summed, gain, stat_ref, s_go, lane)
    x_ref[...] = normed.astype(jnp.bfloat16)

    i_copy.wait()
    d_copy.wait()
    for way in range(LANES - 1):
        i_go(way).wait_recv()
        d_go(way).wait_recv()
        w_go(way).wait_send()
        w_pair(way).wait_send()
        r_go(way).wait_send()
        i_go(way).wait_send()
        d_go(way).wait_send()
        a_go(way).wait_send()
        s_go(way).wait_send()
    for s in range(4):
        first(s, ended, False)

    @pl.when(core == 1)
    def _():
        ahead(1, ended, False)

    def finish(h, _):
        for s in range(4):
            later(h, s, ended, False)
        return 0

    lax.fori_loop(1, 5, finish, 0)


def norm_over_lanes(z, gain, stat_ref, s_go, lane):
    rows, wide = z.shape
    mean = jnp.sum(z, 1, keepdims=True) * (1.0 / wide)
    centre = z - mean
    m2 = jnp.sum(centre * centre, 1, keepdims=True)
    column = lax.broadcasted_iota(jnp.int32, (rows, 128), 1)
    both = jnp.where(column == 0, mean, m2)
    stat_ref[lane] = both.T[:8]
    for way in range(LANES - 1):
        s_go(way).start()
    for way in range(LANES - 1):
        s_go(way).wait_recv()
    means = [stat_ref[j][0:1] for j in range(LANES)]
    m2s = [stat_ref[j][1:2] for j in range(LANES)]
    full = (means[0] + means[1] + means[2] + means[3]) * (1.0 / LANES)
    away = sum((v - full) * (v - full) for v in means)
    spread = (m2s[0] + m2s[1] + m2s[2] + m2s[3] + wide * away) * (1.0 / (wide * LANES))
    scale = lax.rsqrt(spread + 1e-06)
    row = lax.broadcasted_iota(jnp.int32, (128, rows), 0)
    packed = jnp.where(row == 0, full, scale).T
    return (z - packed[:, 0:1]) * packed[:, 1:2] * gain


def front(q_t, keys_values, out_weight, down_proj, resid, info, gain):
    tokens, pair = keys_values.shape
    width = pair // 2
    rows = q_t.shape[1]
    depth, model = out_weight.shape
    wide = model // LANES
    vmem = pl.BlockSpec(memory_space=pltpu.VMEM)
    hbm = pl.BlockSpec(memory_space=pltpu.HBM)
    dma = pltpu.SemaphoreType.DMA
    others = LANES - 1
    return pl.pallas_call(
        front_kernel,
        in_specs=[vmem, vmem, hbm, hbm, hbm, vmem, vmem],
        out_specs=[vmem, vmem, vmem],
        out_shape=[
            jax.ShapeDtypeStruct((tokens, wide), jnp.bfloat16),
            jax.ShapeDtypeStruct((LANES, down_proj.shape[0], wide), jnp.bfloat16),
            jax.ShapeDtypeStruct((LANES, *info.shape), jnp.float32),
        ],
        scratch_shapes=[
            pltpu.VMEM((2, Z_SIZE, X_SIZE, tokens, pair), jnp.bfloat16),
            pltpu.VMEM((1, rows), jnp.float32),
            pltpu.VMEM((1, rows), jnp.float32),
            pltpu.VMEM((width, rows), jnp.float32),
            pltpu.VMEM((LANES, tokens, depth), jnp.bfloat16),
            pltpu.VMEM((LANES, depth, wide), jnp.bfloat16),
            pltpu.VMEM((LANES, resid.shape[0], wide), jnp.bfloat16),
            pltpu.VMEM((LANES, 8, tokens), jnp.float32),
            dma((Z_SIZE, X_SIZE, 5)),
            dma((Z_SIZE, X_SIZE)),
            dma((Z_SIZE, X_SIZE, 2)),
            dma((Z_SIZE, X_SIZE)),
            dma((5,)),
        ]
        + [dma((others,))] * 14,
        compiler_params=pltpu.CompilerParams(
            vmem_limit_bytes=VMEM_LIMIT, collective_id=2, has_side_effects=True
        ),
        cost_estimate=pl.CostEstimate(
            flops=20_000_000_000, bytes_accessed=100_000_000, transcendentals=rows * 16384
        ),
        name="front",
    )(q_t, keys_values, out_weight, down_proj, resid, info, gain)


def half_rows(rows, columns):
    row = lax.broadcasted_iota(jnp.int32, (rows, columns), 0)
    return ((row % 8) < 4).astype(jnp.float32)


def widened(block, left):
    value = block.astype(jnp.float32)
    first = value * left
    return jnp.concatenate([first, value - first], 1).astype(jnp.bfloat16)


def halves_added(value):
    rows, columns = value.shape
    parts = value.reshape(rows // 8, 8, columns)
    return (parts + pltpu.roll(parts, 4, 1)).reshape(rows, columns)


def moe_kernel(
    x1_ref,
    table_ref,
    gain_ref,
    wg_ref,
    wu_ref,
    wd_ref,
    final_ref,
    out_ref,
    ret_ref,
    mixed_ref,
    stat_ref,
    x_ref,
    h_ref,
    y_ref,
    go_send,
    go_recv,
    ring_send,
    ring_recv,
    pass_send,
    pass_recv,
    hid_send,
    hid_recv,
    back_send,
    back_recv,
    s_send,
    s_recv,
    m_send,
    m_recv,
):
    sp = lax.axis_index("sp")
    lane = lax.axis_index("tp")
    core = lax.rem(sp, 2)
    x_at = lax.rem(sp // 2, X_SIZE)
    z_at = sp // (2 * X_SIZE)
    right = lax.rem(lane + 1, LANES)
    left = lax.rem(lane + LANES - 1, LANES)
    far = lax.rem(lane + 2, LANES)
    wide = wd_ref.shape[1]
    half = wide // 2
    deep = wd_ref.shape[0] // LANES
    peers = X_SIZE * 2
    group = 8 * peers
    count = Z_SIZE

    def z_offset(p):
        away = jnp.where(lax.rem(p, 2) == 0, p // 2 + 1, Z_SIZE - (p + 1) // 2)
        return jnp.where(p == count - 1, 0, away)

    def peer(index, sign):
        p = index // peers
        dx = lax.rem(index, peers) // 2
        dc = lax.rem(index, 2)
        z = lax.rem(z_at + sign * z_offset(p) + Z_SIZE, Z_SIZE)
        x = lax.rem(x_at + sign * dx + X_SIZE, X_SIZE)
        c = lax.rem(core + dc, 2)
        return (z * X_SIZE + x) * 2 + c

    def rows_of(index):
        return pl.ds(pl.multiple_of(index * 8, 8), 8)

    def group_rows(p):
        return pl.ds(pl.multiple_of(p * group, group), group)

    barrier = pltpu.get_barrier_semaphore()

    blocks = count * peers
    own_index = (count - 1) * peers

    def others(index, what):
        @pl.when(index != own_index)
        def _():
            what(index)

    def greet(index, _):
        def signal(index):
            pl.semaphore_signal(
                barrier, inc=1, device_id={"sp": peer(index, 1), "tp": lane}, device_id_type=MESH
            )

        others(index, signal)
        return 0

    lax.fori_loop(0, blocks, greet, 0)
    for other in (left, right, far):
        pl.semaphore_signal(
            barrier, inc=1, device_id={"sp": sp, "tp": other}, device_id_type=MESH
        )
    tokens = x1_ref.shape[0]
    spots = lax.broadcasted_iota(jnp.int32, (tokens, blocks * 8), 1).astype(jnp.float32)

    def pick(column):
        return (spots == table_ref[:, column : column + 1]).astype(jnp.float32)

    def placed(first, second, source):
        return lax.dot_general(
            (pick(first) + pick(second)).astype(jnp.bfloat16),
            source,
            (((0,), (0,)), ((), ())),
            preferred_element_type=jnp.float32,
        )

    x1 = x1_ref[...]
    out_ref[:, :wide] = placed(0, 1, x1).astype(jnp.bfloat16)
    out_ref[:, wide:] = (placed(2, 3, x1[:, :half]) + placed(4, 5, x1[:, half:])).astype(
        jnp.bfloat16
    )
    pl.semaphore_wait(barrier, blocks - 1 + LANES - 1)

    def go(index):
        return pltpu.make_async_remote_copy(
            src_ref=out_ref.at[rows_of(index)],
            dst_ref=x_ref.at[lane, rows_of(index)],
            send_sem=go_send.at[index],
            recv_sem=go_recv.at[index],
            device_id={"sp": peer(index, 1), "tp": lane},
            device_id_type=MESH,
        )

    def back(index):
        return pltpu.make_async_remote_copy(
            src_ref=y_ref.at[rows_of(index)],
            dst_ref=ret_ref.at[rows_of(index)],
            send_sem=back_send.at[index],
            recv_sem=back_recv.at[index],
            device_id={"sp": peer(index, -1), "tp": lane},
            device_id_type=MESH,
        )

    def ring(p, way):
        return pltpu.make_async_remote_copy(
            src_ref=x_ref.at[lane, group_rows(p)],
            dst_ref=x_ref.at[lane, group_rows(p)],
            send_sem=ring_send.at[p, way],
            recv_sem=ring_recv.at[p, way],
            device_id={"sp": sp, "tp": right if way == 0 else left},
            device_id_type=MESH,
        )

    def passed(p, way):
        owner = left if way == 0 else right
        rows = pl.ds(pl.multiple_of(p * group + way * (group // 2), group // 2), group // 2)
        return pltpu.make_async_remote_copy(
            src_ref=x_ref.at[owner, rows],
            dst_ref=x_ref.at[owner, rows],
            send_sem=pass_send.at[p, way],
            recv_sem=pass_recv.at[p, way],
            device_id={"sp": sp, "tp": right if way == 0 else left},
            device_id_type=MESH,
        )

    def hid(p, way):
        return pltpu.make_async_remote_copy(
            src_ref=h_ref.at[lane, group_rows(p)],
            dst_ref=h_ref.at[lane, group_rows(p)],
            send_sem=hid_send.at[p, way],
            recv_sem=hid_recv.at[p, way],
            device_id={"sp": sp, "tp": (right, left, far)[way]},
            device_id_type=MESH,
        )

    own_rows = pl.ds(own_index * 8, 8)
    own_in = pltpu.make_async_copy(
        out_ref.at[own_rows], x_ref.at[lane, own_rows], go_recv.at[own_index]
    )
    own_out = pltpu.make_async_copy(
        y_ref.at[own_rows], ret_ref.at[own_rows], back_recv.at[own_index]
    )
    own_in.start()

    def send_one(index, _):
        others(index, lambda i: go(i).start())
        return 0

    lax.fori_loop(0, blocks, send_one, 0)

    def hidden_of(p):
        rows = group_rows(p)
        left_half = half_rows(group, half)
        gate = None
        up = None
        for j in range(LANES):
            lhs = jnp.concatenate(
                [x_ref[j, rows, :wide], widened(x_ref[j, rows, wide:], left_half)], 0
            )
            g = jnp.dot(
                lhs, wg_ref[j * wide : (j + 1) * wide, :], preferred_element_type=jnp.float32
            )
            u = jnp.dot(
                lhs, wu_ref[j * wide : (j + 1) * wide, :], preferred_element_type=jnp.float32
            )
            gate = g if gate is None else gate + g
            up = u if up is None else up + u
        gate = jnp.concatenate([gate[:group], halves_added(gate[group:])], 0)
        up = jnp.concatenate([up[:group], halves_added(up[group:])], 0)
        hidden = gate / (1.0 + jnp.exp(-gate)) * up
        low = hidden[group:, : deep // 2]
        high = hidden[group:, deep // 2 :]
        narrow = jnp.where(half_rows(group, deep // 2) > 0.0, low, high)
        h_ref[lane, rows, :deep] = hidden[:group].astype(jnp.bfloat16)
        h_ref[lane, rows, deep:] = narrow.astype(jnp.bfloat16)

    def output_of(p):
        rows = group_rows(p)
        left_half = half_rows(group, deep // 2)
        total_a = None
        total_b = None
        for j in range(LANES):
            lhs = jnp.concatenate(
                [h_ref[j, rows, :deep], widened(h_ref[j, rows, deep:], left_half)], 0
            )
            z = jnp.dot(
                lhs, wd_ref[j * deep : (j + 1) * deep, :], preferred_element_type=jnp.float32
            )
            a = z[:group].astype(jnp.bfloat16).astype(jnp.float32)
            b = halves_added(z[group:]).astype(jnp.bfloat16).astype(jnp.float32)
            total_a = a if total_a is None else total_a + a
            total_b = b if total_b is None else total_b + b
        narrow = jnp.where(half_rows(group, half) > 0.0, total_b[:, :half], total_b[:, half:])
        y_ref[rows, :wide] = total_a.astype(jnp.bfloat16)
        y_ref[rows, wide:] = narrow.astype(jnp.bfloat16)

    def step(t, _):
        @pl.when(t < count)
        def _():
            @pl.when(t == count - 1)
            def _():
                own_in.wait()

            def arrived(i, _):
                others(t * peers + i, lambda index: go(index).wait_recv())
                return 0

            lax.fori_loop(0, peers, arrived, 0)
            ring(t, 0).start()
            ring(t, 1).start()

        @pl.when((t >= 1) & (t < count + 1))
        def _():
            ring(t - 1, 0).wait_recv()
            passed(t - 1, 0).start()
            ring(t - 1, 1).wait_recv()
            passed(t - 1, 1).start()

        @pl.when((t >= 2) & (t < count + 2))
        def _():
            passed(t - 2, 0).wait_recv()
            passed(t - 2, 1).wait_recv()
            hidden_of(t - 2)
            for way in range(LANES - 1):
                hid(t - 2, way).start()

        @pl.when(t >= 3)
        def _():
            for way in range(LANES - 1):
                hid(t - 3, way).wait_recv()
            output_of(t - 3)

            @pl.when(t == count + 2)
            def _():
                own_out.start()

            def send_back(i, _):
                others((t - 3) * peers + i, lambda index: back(index).start())
                return 0

            lax.fori_loop(0, peers, send_back, 0)

        return 0

    lax.fori_loop(0, count + 3, step, 0)
    own_out.wait()

    def finish(index, _):
        def ended(index):
            go(index).wait_send()
            back(index).wait_send()
            back(index).wait_recv()

        others(index, ended)
        return 0

    lax.fori_loop(0, blocks, finish, 0)

    moe = None
    for k in range(2):

        def chosen(column, source):
            return jnp.dot(
                pick(column + k).astype(jnp.bfloat16), source, preferred_element_type=jnp.float32
            )

        expert_out = chosen(0, ret_ref[:, :wide]) + jnp.concatenate(
            [chosen(2, ret_ref[:, wide:]), chosen(4, ret_ref[:, wide:])], 1
        )
        term = table_ref[:, 6 + k : 7 + k] * expert_out
        moe = term if moe is None else moe + term
    mixed = deep_alpha * x1_ref[...].astype(jnp.float32) + moe
    lanes_of = (right, left, far)

    def s_go(way):
        return pltpu.make_async_remote_copy(
            src_ref=stat_ref.at[lane],
            dst_ref=stat_ref.at[lane],
            send_sem=s_send.at[way],
            recv_sem=s_recv.at[way],
            device_id={"sp": sp, "tp": lanes_of[way]},
            device_id_type=MESH,
        )

    own_tokens = tokens // LANES

    def m_go(way):
        rows = pl.ds(pl.multiple_of(lanes_of[way] * own_tokens, own_tokens), own_tokens)
        return pltpu.make_async_remote_copy(
            src_ref=mixed_ref.at[rows],
            dst_ref=final_ref.at[:, pl.ds(pl.multiple_of(lane * wide, wide), wide)],
            send_sem=m_send.at[way],
            recv_sem=m_recv.at[way],
            device_id={"sp": sp, "tp": lanes_of[way]},
            device_id_type=MESH,
        )

    gain = gain_ref[:, pl.ds(pl.multiple_of(lane * wide, wide), wide)]
    mixed_ref[...] = norm_over_lanes(mixed, gain, stat_ref, s_go, lane).astype(jnp.bfloat16)
    for way in range(LANES - 1):
        m_go(way).start()
    final_ref[:, pl.ds(pl.multiple_of(lane * wide, wide), wide)] = mixed_ref[
        pl.ds(pl.multiple_of(lane * own_tokens, own_tokens), own_tokens)
    ]
    for way in range(LANES - 1):
        s_go(way).wait_send()
        m_go(way).wait_recv()
        m_go(way).wait_send()

    def finish_group(p, _):
        for way in range(2):
            ring(p, way).wait_send()
            passed(p, way).wait_send()
        for way in range(LANES - 1):
            hid(p, way).wait_send()
        return 0

    lax.fori_loop(0, count, finish_group, 0)


def moe_layer(x_one, table, gain, w_gate, w_up, w_down):
    tokens, wide = x_one.shape
    rows, columns = Z_SIZE * X_SIZE * 2 * 8, wide * 3 // 2
    hidden = w_gate.shape[1]
    blocks = rows // 8
    vmem = pl.BlockSpec(memory_space=pltpu.VMEM)
    dma = pltpu.SemaphoreType.DMA
    return pl.pallas_call(
        moe_kernel,
        in_specs=[vmem] * 6,
        out_specs=vmem,
        out_shape=jax.ShapeDtypeStruct((tokens // LANES, wide * LANES), jnp.bfloat16),
        scratch_shapes=[
            pltpu.VMEM((rows, columns), jnp.bfloat16),
            pltpu.VMEM((rows, columns), jnp.bfloat16),
            pltpu.VMEM((tokens, wide), jnp.bfloat16),
            pltpu.VMEM((LANES, 8, tokens), jnp.float32),
            pltpu.VMEM((LANES, rows, columns), jnp.bfloat16),
            pltpu.VMEM((LANES, rows, hidden * 3 // 2), jnp.bfloat16),
            pltpu.VMEM((rows, columns), jnp.bfloat16),
            dma((blocks,)),
            dma((blocks,)),
            dma((Z_SIZE, 2)),
            dma((Z_SIZE, 2)),
            dma((Z_SIZE, 2)),
            dma((Z_SIZE, 2)),
            dma((Z_SIZE, LANES - 1)),
            dma((Z_SIZE, LANES - 1)),
            dma((blocks,)),
            dma((blocks,)),
            dma((LANES - 1,)),
            dma((LANES - 1,)),
            dma((LANES - 1,)),
            dma((LANES - 1,)),
        ],
        compiler_params=pltpu.CompilerParams(
            vmem_limit_bytes=VMEM_LIMIT, collective_id=1, has_side_effects=True
        ),
        cost_estimate=pl.CostEstimate(
            flops=12 * LANES * rows * 1024 * hidden,
            bytes_accessed=200_000_000,
            transcendentals=0,
        ),
        name="experts",
    )(x_one, table, gain, w_gate, w_up, w_down)


def per_device(
    resid,
    queries,
    keys,
    values,
    q_gain,
    key_norm_gain,
    out_weight,
    norm1_gain,
    norm2_gain,
    expert_ids,
    group_weight,
    expert_weight,
    gate_proj,
    up_proj,
    down_proj,
):
    tokens = queries.shape[0]
    width = q_gain.shape[0]
    heads = queries.shape[1] // width
    lanes = lax.axis_size("tp")
    sp_count = lax.axis_size("sp")
    lane = lax.axis_index("tp")
    own = tokens // lanes
    model_width = resid.shape[1]
    part = model_width // lanes

    positions = lax.axis_index("sp") * tokens + jnp.arange(tokens, dtype=jnp.int32)
    rotated_keys = apply_rotary_heads(keys.reshape(tokens, 1, width), key_norm_gain, positions)
    both = jnp.concatenate([rotated_keys.reshape(tokens, width), values], 1)
    gates_own = (
        group_weight[:, None] * expert_weight / jnp.sum(expert_weight, -1, keepdims=True)
    )
    top = expert_ids.shape[1]
    sp = lax.axis_index("sp")
    flat = expert_ids.reshape(-1)
    one_hot = (flat[:, None] == jnp.arange(sp_count, dtype=jnp.int32)).astype(jnp.int32)
    earlier = jnp.cumsum(one_hot, 0) - one_hot
    rank = jnp.sum(earlier * one_hot, 1)
    dz = (flat // (2 * X_SIZE) - sp // (2 * X_SIZE)) % Z_SIZE
    dx = (flat // 2 - sp // 2) % X_SIZE
    dc = (flat - sp) % 2
    near = jnp.where(dz <= Z_SIZE // 2, 2 * dz - 2, 2 * (Z_SIZE - dz) - 1)
    near = jnp.where(dz == 0, Z_SIZE - 1, near)
    target = ((near * X_SIZE + dx) * 2 + dc) * 8
    place = lane * CAP + rank
    row_a = jnp.where(place < 8, target + place, -1)
    row_b = jnp.where(place < 8, -1, target + place - 8)
    row_c = jnp.where(place < 8, -1, target + place - 4)
    info = jnp.concatenate(
        [v.reshape(own, top).astype(jnp.float32) for v in (row_a, row_b, row_c)]
        + [gates_own, jnp.zeros((own, 128 - 4 * top), jnp.float32)],
        1,
    )

    q_rot = apply_rotary_heads(queries.reshape(tokens, heads, width), q_gain, positions)
    factor = np.float32(np.log2(np.e) * width**-0.5)
    scaled = q_rot.astype(jnp.float32) * factor
    coarse = lax.reduce_precision(scaled, 8, 7)
    fine = (scaled - coarse).astype(jnp.bfloat16)
    pair = jnp.concatenate([coarse.astype(jnp.bfloat16), fine], -1)
    q_t = pair.transpose(2, 1, 0).reshape(2 * width, heads * tokens)
    x_one, down_slice, table = front(
        q_t, both, out_weight, down_proj[0], resid, info, norm1_gain[None]
    )
    return moe_layer(
        x_one,
        table.reshape(tokens, -1),
        norm2_gain[None],
        gate_proj[0],
        up_proj[0],
        down_slice.reshape(-1, part),
    )


def solution(mesh):
    in_specs = (
        P(("sp", "tp"), None),
        P("sp", "tp"),
        P("sp", "tp"),
        P("sp", "tp"),
        P(),
        P(),
        P("tp", None),
        P(),
        P(),
        P(("sp", "tp"), None),
        P(("sp", "tp")),
        P(("sp", "tp"), None),
        P("sp", None, "tp"),
        P("sp", None, "tp"),
        P("sp", "tp", None),
    )
    out_specs = P(("sp", "tp"), None)
    return jax.shard_map(
        per_device, mesh=mesh, in_specs=in_specs, out_specs=out_specs, check_vma=False
    )
```

```python
import jax
import jax.numpy as jnp
import numpy as np
from jax import lax
from jax.experimental import pallas as pl
from jax.experimental.pallas import tpu as pltpu
from jax.sharding import PartitionSpec as P

GRID_W = 64
CAP = 3
QUERY_TILE = 512

deep_alpha = 2.0**0.5
rope_theta = 10000.0
VMEM_LIMIT = 60 * 1024 * 1024
MESH = pl.DeviceIdType.MESH
Z_SIZE = 8
X_SIZE = 4
LANES = 4
GROUPS = 16


def apply_rotary_heads(block, gain, grid_positions):
    values32 = block.astype(jnp.float32)
    normed = values32 * lax.rsqrt(jnp.mean(values32 * values32, -1, keepdims=True) + 1e-06) * gain
    half = normed.shape[-1] // 2
    inv_freq = rope_theta ** (-jnp.arange(0, half, 2, dtype=jnp.float32) / half)
    grid_row = (grid_positions // GRID_W).astype(jnp.float32)
    grid_col = (grid_positions % GRID_W).astype(jnp.float32)
    angle = jnp.concatenate([grid_row[:, None] * inv_freq, grid_col[:, None] * inv_freq], -1)[
        :, None, :
    ]
    cosine = jnp.cos(angle)
    sine = jnp.sin(angle)
    first = normed[..., :half]
    second = normed[..., half:]
    turned = jnp.concatenate([first * cosine - second * sine, first * sine + second * cosine], -1)
    return turned.astype(jnp.bfloat16)


def front_kernel(
    qt_ref,
    own_ref,
    w_ref,
    wd_ref,
    resid_ref,
    info_ref,
    gain_ref,
    x_ref,
    down_ref,
    table_ref,
    kv_ref,
    m_ref,
    l_ref,
    acc_ref,
    attn_ref,
    out_ref,
    res_ref,
    stat_ref,
    tx,
    rx_full,
    rx_half,
    rx_core,
    load_sem,
    w_send,
    w_recv,
    w_pair_send,
    w_pair_recv,
    d_send,
    d_recv,
    r_send,
    r_recv,
    i_send,
    i_recv,
    a_send,
    a_recv,
    s_send,
    s_recv,
):
    sp = lax.axis_index("sp")
    lane = lax.axis_index("tp")
    core = lax.rem(sp, 2)
    x_at = lax.rem(sp // 2, X_SIZE)
    z_at = sp // (2 * X_SIZE)
    partner = sp + 1 - 2 * core
    block = own_ref.shape[0]
    width = own_ref.shape[1] // 2
    rows = qt_ref.shape[1]
    heads = rows // block
    wide = x_ref.shape[1]
    lane_rows = res_ref.shape[1]
    depth = out_ref.shape[1]
    lanes_of = [lax.rem(lane + 1, LANES), lax.rem(lane + LANES - 1, LANES), lax.rem(lane + 2, LANES)]
    froms = [lanes_of[1], lanes_of[0], lanes_of[2]]

    def sp_of(z, x, c):
        return (lax.rem(z + 2 * Z_SIZE, Z_SIZE) * X_SIZE + lax.rem(x + 2 * X_SIZE, X_SIZE)) * 2 + c

    ways = (
        sp_of(z_at + 1, x_at, core),
        sp_of(z_at - 1, x_at, core),
        sp_of(z_at, x_at + 1, core),
        sp_of(z_at, x_at - 1, core),
        partner,
    )
    barrier = pltpu.get_barrier_semaphore()
    for way in range(5):
        pl.semaphore_signal(
            barrier, inc=1, device_id={"sp": ways[way], "tp": lane}, device_id_type=MESH
        )
    for other in lanes_of:
        pl.semaphore_signal(
            barrier, inc=1, device_id={"sp": sp, "tp": other}, device_id_type=MESH
        )

    own_copy = pltpu.make_async_copy(own_ref, kv_ref.at[core, z_at, x_at], load_sem.at[0])
    w_copy = pltpu.make_async_copy(
        w_ref.at[:, pl.ds(pl.multiple_of(lane * wide, wide), wide)], out_ref.at[lane], load_sem.at[1]
    )
    d_copy = pltpu.make_async_copy(
        wd_ref.at[:, pl.ds(pl.multiple_of(lane * wide, wide), wide)], down_ref.at[lane], load_sem.at[2]
    )
    r_copy = pltpu.make_async_copy(
        resid_ref.at[:, pl.ds(pl.multiple_of(lane * wide, wide), wide)], res_ref.at[lane], load_sem.at[3]
    )
    i_copy = pltpu.make_async_copy(info_ref, table_ref.at[lane], load_sem.at[4])
    own_copy.start()

    def to_lane(src, dst, send, recv, way):
        return pltpu.make_async_remote_copy(
            src_ref=src,
            dst_ref=dst,
            send_sem=send.at[way],
            recv_sem=recv.at[way],
            device_id={"sp": sp, "tp": lanes_of[way]},
            device_id_type=MESH,
        )

    def columns(way):
        return pl.ds(pl.multiple_of(lanes_of[way] * wide, wide), wide)

    part_rows = depth // 2
    half = pl.ds(pl.multiple_of(core * part_rows, part_rows), part_rows)

    def w_go(way):
        return to_lane(w_ref.at[half, columns(way)], out_ref.at[lane, half], w_send, w_recv, way)

    def w_pair(way):
        return pltpu.make_async_remote_copy(
            src_ref=out_ref.at[froms[way], half],
            dst_ref=out_ref.at[froms[way], half],
            send_sem=w_pair_send.at[way],
            recv_sem=w_pair_recv.at[way],
            device_id={"sp": partner, "tp": lane},
            device_id_type=MESH,
        )

    def d_go(way):
        return to_lane(wd_ref.at[:, columns(way)], down_ref.at[lane], d_send, d_recv, way)

    def r_go(way):
        return to_lane(resid_ref.at[:, columns(way)], res_ref.at[lane], r_send, r_recv, way)

    def i_go(way):
        return to_lane(info_ref, table_ref.at[lane], i_send, i_recv, way)

    def a_go(way):
        return to_lane(attn_ref.at[lane], attn_ref.at[lane], a_send, a_recv, way)

    def s_go(way):
        return to_lane(stat_ref.at[lane], stat_ref.at[lane], s_send, s_recv, way)

    def send(cls, zz, xx, way, piece=None):
        if piece is None:
            at = kv_ref.at[cls, zz, xx]
            recv = rx_core.at[zz, xx] if way == 4 else rx_full.at[zz, xx]
        else:
            at = kv_ref.at[cls, zz, xx, pl.ds(piece * (block // 2), block // 2)]
            recv = rx_half.at[zz, xx, piece]
        return pltpu.make_async_remote_copy(
            src_ref=at,
            dst_ref=at,
            send_sem=tx.at[zz, xx, way],
            recv_sem=recv,
            device_id={"sp": ways[way], "tp": lane},
            device_id_type=MESH,
        )

    def wait_block(zz, xx, halves):
        if halves:
            send(core, zz, xx, 0, 0).wait_recv()
            send(core, zz, xx, 0, 1).wait_recv()
        else:
            send(core, zz, xx, 0).wait_recv()

    def z_of(d):
        return lax.rem(z_at + d + Z_SIZE, Z_SIZE)

    x_order = [
        x_at,
        lax.rem(x_at + X_SIZE - 1, X_SIZE),
        lax.rem(x_at + 1, X_SIZE),
        lax.rem(x_at + 2, X_SIZE),
    ]

    def along_x(zz, s, act):
        if s == 0:
            act(send(core, zz, x_order[0], 2))
            act(send(core, zz, x_order[0], 3))
        elif s == 1:
            act(send(core, zz, x_order[1], 2, 0))
        elif s == 2:
            act(send(core, zz, x_order[2], 3, 1))

    def along_z(h, xx, side, act):
        zz = z_of(-h if side == 0 else h)

        @pl.when(h < 3)
        def _():
            act(send(core, zz, xx, side))

        @pl.when(h == 3)
        def _():
            act(send(core, zz, xx, side, side))

    def first(s, act, wait):
        xx = x_order[s]
        if wait and s > 0:
            wait_block(z_at, xx, s == 3)
        along_x(z_at, s, act)

        if s == 0:
            act(send(core, z_at, xx, 0))
            act(send(core, z_at, xx, 1))
        else:

            @pl.when(core == 0)
            def _():
                act(send(core, z_at, xx, 0))
                act(send(core, z_at, xx, 1))

        act(send(core, z_at, xx, 4))

    def later(h, s, act, wait):
        xx = x_order[s]

        @pl.when(core == 0)
        def _():
            @pl.when(h < 4)
            def _():
                for side in range(2):
                    zz = z_of(-h if side == 0 else h)
                    if wait:
                        wait_block(zz, xx, False)
                    along_z(h, xx, side, act)
                    act(send(core, zz, xx, 4))

            @pl.when(h == 4)
            def _():
                zz = z_of(4)
                if wait:
                    wait_block(zz, xx, True)
                act(send(core, zz, xx, 4))

        @pl.when(core == 1)
        def _():
            if s == 0:

                @pl.when(h < 4)
                def _():
                    ahead(h + 1, act, wait)
            else:

                @pl.when(h < 4)
                def _():
                    for side in range(2):
                        zz = z_of(-h if side == 0 else h)
                        if wait:
                            wait_block(zz, xx, s == 3)
                        along_x(zz, s, act)
                        act(send(core, zz, xx, 4))

                @pl.when(h == 4)
                def _():
                    zz = z_of(4)
                    if wait:
                        wait_block(zz, xx, s == 3)
                    along_x(zz, s, act)
                    act(send(core, zz, xx, 4))

    def ahead(h, act, wait):
        @pl.when(h < 4)
        def _():
            for side in range(2):
                zz = z_of(-h if side == 0 else h)
                if wait:
                    wait_block(zz, x_at, False)
                along_z(h, x_at, side, act)
                along_x(zz, 0, act)
                act(send(core, zz, x_at, 4))

        @pl.when(h == 4)
        def _():
            zz = z_of(4)
            if wait:
                wait_block(zz, x_at, True)
            along_x(zz, 0, act)
            act(send(core, zz, x_at, 4))

    def start(copy):
        copy.start()

    def ended(copy):
        copy.wait_send()

    m_ref[...] = jnp.full_like(m_ref, -1e30)
    l_ref[...] = jnp.zeros_like(l_ref)
    acc_ref[...] = jnp.zeros_like(acc_ref)
    own_copy.wait()
    pl.semaphore_wait(barrier, 5 + LANES - 1)
    first(0, start, True)
    for way in range(LANES - 1):
        i_go(way).start()
    for way in range(LANES - 1):
        w_go(way).start()
    for way in range(LANES - 1):
        r_go(way).start()
    for way in range(LANES - 1):
        d_go(way).start()
    w_copy.start()
    r_copy.start()
    d_copy.start()
    i_copy.start()

    @pl.when(core == 1)
    def _():
        ahead(1, start, True)

    for s in range(1, 4):
        first(s, start, True)

    tile = min(QUERY_TILE, rows)
    keys = X_SIZE * block

    def attend(cls, zz):
        both = kv_ref[cls, zz].reshape(keys, 2 * width)
        k = both[:, :width]
        k_twice = jnp.concatenate([k, k], 1)
        v_t = both[:, width:].T

        def scores(t):
            return jnp.dot(
                k_twice, qt_ref[:, t * tile : (t + 1) * tile], preferred_element_type=jnp.float32
            )

        s = scores(0)
        for t in range(rows // tile):
            following = scores(t + 1) if t + 1 < rows // tile else None
            at = slice(t * tile, (t + 1) * tile)
            m_old = m_ref[:, at]
            m_new = jnp.maximum(m_old, jnp.max(s, 0, keepdims=True))
            shrink = jnp.exp2(m_old - m_new)
            p = jnp.exp2(s - m_new)
            l_ref[:, at] = l_ref[:, at] * shrink + jnp.sum(p, 0, keepdims=True)
            m_ref[:, at] = m_new
            pv = jnp.dot(v_t, p.astype(jnp.bfloat16), preferred_element_type=jnp.float32)
            acc_ref[:, at] = acc_ref[:, at] * shrink + pv
            s = following

    def slot(i, _):
        dist = jnp.where(i < 2, 0, (i - 2) // 4 + 1)
        turn = lax.rem(i + 2, 4)
        ours = jnp.where((dist == 0) | (dist == 4), lax.rem(i, 2) == 0, turn < 2)
        side = jnp.where((dist == 0) | (dist == 4), 1, lax.rem(i, 2))
        zz = z_of(jnp.where(side == 0, -dist, dist))
        cls = jnp.where(ours, core, 1 - core)

        @pl.when(cls != core)
        def _():
            for xx in range(X_SIZE):
                pltpu.make_async_remote_copy(
                    src_ref=kv_ref.at[cls, zz, xx],
                    dst_ref=kv_ref.at[cls, zz, xx],
                    send_sem=tx.at[zz, xx, 4],
                    recv_sem=rx_core.at[zz, xx],
                    device_id={"sp": partner, "tp": lane},
                    device_id_type=MESH,
                ).wait_recv()

        attend(cls, zz)
        for s in range(4):

            @pl.when(((i < 2) & (s // 2 == i)) | ((i >= 2) & (i < 14) & (turn == s)))
            def _(s=s):
                later(dist + 1, s, start, True)

        @pl.when(i == 12)
        def _():
            for way in range(LANES - 1):
                w_go(way).wait_recv()
                w_pair(way).start()

        return 0

    lax.fori_loop(0, 16, slot, 0)

    for h in range(heads):
        at = slice(h * block, (h + 1) * block)
        out = acc_ref[:, at] / l_ref[:, at]
        attn_ref[lane, :, h * width : (h + 1) * width] = out.T.astype(jnp.bfloat16)
    for way in range(LANES - 1):
        a_go(way).start()
    w_copy.wait()
    for way in range(LANES - 1):
        w_pair(way).wait_recv()
    total = jnp.dot(attn_ref[lane], out_ref[lane], preferred_element_type=jnp.float32)
    for way in range(LANES - 1):
        a_go(way).wait_recv()
        total = total + jnp.dot(
            attn_ref[froms[way]], out_ref[froms[way]], preferred_element_type=jnp.float32
        )
    r_copy.wait()
    for way in range(LANES - 1):
        r_go(way).wait_recv()
    summed = deep_alpha * res_ref[...].reshape(LANES * lane_rows, wide).astype(jnp.float32)
    summed = summed + total.astype(jnp.bfloat16).astype(jnp.float32)
    gain = gain_ref[:, pl.ds(pl.multiple_of(lane * wide, wide), wide)]
    normed = norm_over_lanes(summed, gain, stat_ref, s_go, lane)
    x_ref[...] = normed.astype(jnp.bfloat16)

    i_copy.wait()
    d_copy.wait()
    for way in range(LANES - 1):
        i_go(way).wait_recv()
        d_go(way).wait_recv()
        w_go(way).wait_send()
        w_pair(way).wait_send()
        r_go(way).wait_send()
        i_go(way).wait_send()
        d_go(way).wait_send()
        a_go(way).wait_send()
        s_go(way).wait_send()
    for s in range(4):
        first(s, ended, False)

    @pl.when(core == 1)
    def _():
        ahead(1, ended, False)

    def finish(h, _):
        for s in range(4):
            later(h, s, ended, False)
        return 0

    lax.fori_loop(1, 5, finish, 0)


def norm_over_lanes(z, gain, stat_ref, s_go, lane):
    rows, wide = z.shape
    mean = jnp.sum(z, 1, keepdims=True) * (1.0 / wide)
    centre = z - mean
    m2 = jnp.sum(centre * centre, 1, keepdims=True)
    column = lax.broadcasted_iota(jnp.int32, (rows, 128), 1)
    both = jnp.where(column == 0, mean, m2)
    stat_ref[lane] = both.T[:8]
    for way in range(LANES - 1):
        s_go(way).start()
    for way in range(LANES - 1):
        s_go(way).wait_recv()
    means = [stat_ref[j][0:1] for j in range(LANES)]
    m2s = [stat_ref[j][1:2] for j in range(LANES)]
    full = (means[0] + means[1] + means[2] + means[3]) * (1.0 / LANES)
    away = sum((v - full) * (v - full) for v in means)
    spread = (m2s[0] + m2s[1] + m2s[2] + m2s[3] + wide * away) * (1.0 / (wide * LANES))
    scale = lax.rsqrt(spread + 1e-06)
    row = lax.broadcasted_iota(jnp.int32, (128, rows), 0)
    packed = jnp.where(row == 0, full, scale).T
    return (z - packed[:, 0:1]) * packed[:, 1:2] * gain


def front(q_t, keys_values, out_weight, down_proj, resid, info, gain):
    tokens, pair = keys_values.shape
    width = pair // 2
    rows = q_t.shape[1]
    depth, model = out_weight.shape
    wide = model // LANES
    vmem = pl.BlockSpec(memory_space=pltpu.VMEM)
    hbm = pl.BlockSpec(memory_space=pltpu.HBM)
    dma = pltpu.SemaphoreType.DMA
    others = LANES - 1
    return pl.pallas_call(
        front_kernel,
        in_specs=[vmem, vmem, hbm, hbm, hbm, vmem, vmem],
        out_specs=[vmem, vmem, vmem],
        out_shape=[
            jax.ShapeDtypeStruct((tokens, wide), jnp.bfloat16),
            jax.ShapeDtypeStruct((LANES, down_proj.shape[0], wide), jnp.bfloat16),
            jax.ShapeDtypeStruct((LANES, *info.shape), jnp.float32),
        ],
        scratch_shapes=[
            pltpu.VMEM((2, Z_SIZE, X_SIZE, tokens, pair), jnp.bfloat16),
            pltpu.VMEM((1, rows), jnp.float32),
            pltpu.VMEM((1, rows), jnp.float32),
            pltpu.VMEM((width, rows), jnp.float32),
            pltpu.VMEM((LANES, tokens, depth), jnp.bfloat16),
            pltpu.VMEM((LANES, depth, wide), jnp.bfloat16),
            pltpu.VMEM((LANES, resid.shape[0], wide), jnp.bfloat16),
            pltpu.VMEM((LANES, 8, tokens), jnp.float32),
            dma((Z_SIZE, X_SIZE, 5)),
            dma((Z_SIZE, X_SIZE)),
            dma((Z_SIZE, X_SIZE, 2)),
            dma((Z_SIZE, X_SIZE)),
            dma((5,)),
        ]
        + [dma((others,))] * 14,
        compiler_params=pltpu.CompilerParams(
            vmem_limit_bytes=VMEM_LIMIT, collective_id=2, has_side_effects=True
        ),
        cost_estimate=pl.CostEstimate(
            flops=20_000_000_000, bytes_accessed=100_000_000, transcendentals=rows * 16384
        ),
        name="front",
    )(q_t, keys_values, out_weight, down_proj, resid, info, gain)


def half_rows(rows, columns):
    row = lax.broadcasted_iota(jnp.int32, (rows, columns), 0)
    return ((row % 8) < 4).astype(jnp.float32)


def widened(block, left):
    value = block.astype(jnp.float32)
    first = value * left
    return jnp.concatenate([first, value - first], 1).astype(jnp.bfloat16)


def halves_added(value):
    rows, columns = value.shape
    parts = value.reshape(rows // 8, 8, columns)
    return (parts + pltpu.roll(parts, 4, 1)).reshape(rows, columns)


def moe_kernel(
    x1_ref,
    table_ref,
    gain_ref,
    wg_ref,
    wu_ref,
    wd_ref,
    final_ref,
    out_ref,
    ret_ref,
    mixed_ref,
    stat_ref,
    x_ref,
    h_ref,
    y_ref,
    go_send,
    go_recv,
    ring_send,
    ring_recv,
    pass_send,
    pass_recv,
    hid_send,
    hid_recv,
    back_send,
    back_recv,
    s_send,
    s_recv,
    m_send,
    m_recv,
):
    sp = lax.axis_index("sp")
    lane = lax.axis_index("tp")
    core = lax.rem(sp, 2)
    x_at = lax.rem(sp // 2, X_SIZE)
    z_at = sp // (2 * X_SIZE)
    right = lax.rem(lane + 1, LANES)
    left = lax.rem(lane + LANES - 1, LANES)
    far = lax.rem(lane + 2, LANES)
    wide = wd_ref.shape[1]
    half = wide // 2
    deep = wd_ref.shape[0] // LANES
    peers = X_SIZE * 2
    blocks = Z_SIZE * peers
    count = GROUPS
    members = blocks // count
    group = 8 * members

    def z_offset(p):
        away = jnp.where(lax.rem(p, 2) == 0, p // 2 + 1, Z_SIZE - (p + 1) // 2)
        return jnp.where(p == Z_SIZE - 1, 0, away)

    def peer(index, sign):
        p = index // peers
        dx = lax.rem(index, peers) // 2
        dc = lax.rem(index, 2)
        z = lax.rem(z_at + sign * z_offset(p) + Z_SIZE, Z_SIZE)
        x = lax.rem(x_at + sign * dx + X_SIZE, X_SIZE)
        c = lax.rem(core + dc, 2)
        return (z * X_SIZE + x) * 2 + c

    def rows_of(index):
        return pl.ds(pl.multiple_of(index * 8, 8), 8)

    def group_rows(p):
        return pl.ds(pl.multiple_of(p * group, group), group)

    barrier = pltpu.get_barrier_semaphore()

    own_index = (Z_SIZE - 1) * peers
    own_group = own_index // members

    def others(index, what):
        @pl.when(index != own_index)
        def _():
            what(index)

    def greet(index, _):
        def signal(index):
            pl.semaphore_signal(
                barrier, inc=1, device_id={"sp": peer(index, 1), "tp": lane}, device_id_type=MESH
            )

        others(index, signal)
        return 0

    lax.fori_loop(0, blocks, greet, 0)
    for other in (left, right, far):
        pl.semaphore_signal(
            barrier, inc=1, device_id={"sp": sp, "tp": other}, device_id_type=MESH
        )
    tokens = x1_ref.shape[0]
    spots = lax.broadcasted_iota(jnp.int32, (tokens, blocks * 8), 1).astype(jnp.float32)

    def pick(column):
        return (spots == table_ref[:, column : column + 1]).astype(jnp.float32)

    def placed(first, second, source):
        return lax.dot_general(
            (pick(first) + pick(second)).astype(jnp.bfloat16),
            source,
            (((0,), (0,)), ((), ())),
            preferred_element_type=jnp.float32,
        )

    x1 = x1_ref[...]
    out_ref[:, :wide] = placed(0, 1, x1).astype(jnp.bfloat16)
    out_ref[:, wide:] = (placed(2, 3, x1[:, :half]) + placed(4, 5, x1[:, half:])).astype(
        jnp.bfloat16
    )
    pl.semaphore_wait(barrier, blocks - 1 + LANES - 1)

    def go(index):
        return pltpu.make_async_remote_copy(
            src_ref=out_ref.at[rows_of(index)],
            dst_ref=x_ref.at[lane, rows_of(index)],
            send_sem=go_send.at[index],
            recv_sem=go_recv.at[index],
            device_id={"sp": peer(index, 1), "tp": lane},
            device_id_type=MESH,
        )

    def back(index):
        return pltpu.make_async_remote_copy(
            src_ref=y_ref.at[rows_of(index)],
            dst_ref=ret_ref.at[rows_of(index)],
            send_sem=back_send.at[index],
            recv_sem=back_recv.at[index],
            device_id={"sp": peer(index, -1), "tp": lane},
            device_id_type=MESH,
        )

    def ring(p, way):
        return pltpu.make_async_remote_copy(
            src_ref=x_ref.at[lane, group_rows(p)],
            dst_ref=x_ref.at[lane, group_rows(p)],
            send_sem=ring_send.at[p, way],
            recv_sem=ring_recv.at[p, way],
            device_id={"sp": sp, "tp": right if way == 0 else left},
            device_id_type=MESH,
        )

    def passed(p, way):
        owner = left if way == 0 else right
        rows = pl.ds(pl.multiple_of(p * group + way * (group // 2), group // 2), group // 2)
        return pltpu.make_async_remote_copy(
            src_ref=x_ref.at[owner, rows],
            dst_ref=x_ref.at[owner, rows],
            send_sem=pass_send.at[p, way],
            recv_sem=pass_recv.at[p, way],
            device_id={"sp": sp, "tp": right if way == 0 else left},
            device_id_type=MESH,
        )

    def hid(p, way):
        return pltpu.make_async_remote_copy(
            src_ref=h_ref.at[lane, group_rows(p)],
            dst_ref=h_ref.at[lane, group_rows(p)],
            send_sem=hid_send.at[p, way],
            recv_sem=hid_recv.at[p, way],
            device_id={"sp": sp, "tp": (right, left, far)[way]},
            device_id_type=MESH,
        )

    own_rows = pl.ds(own_index * 8, 8)
    own_in = pltpu.make_async_copy(
        out_ref.at[own_rows], x_ref.at[lane, own_rows], go_recv.at[own_index]
    )
    own_out = pltpu.make_async_copy(
        y_ref.at[own_rows], ret_ref.at[own_rows], back_recv.at[own_index]
    )
    own_in.start()

    def send_one(index, _):
        others(index, lambda i: go(i).start())
        return 0

    lax.fori_loop(0, blocks, send_one, 0)

    def hidden_of(p):
        rows = group_rows(p)
        left_half = half_rows(group, half)
        gate = None
        up = None
        for j in range(LANES):
            lhs = jnp.concatenate(
                [x_ref[j, rows, :wide], widened(x_ref[j, rows, wide:], left_half)], 0
            )
            g = jnp.dot(
                lhs, wg_ref[j * wide : (j + 1) * wide, :], preferred_element_type=jnp.float32
            )
            u = jnp.dot(
                lhs, wu_ref[j * wide : (j + 1) * wide, :], preferred_element_type=jnp.float32
            )
            gate = g if gate is None else gate + g
            up = u if up is None else up + u
        gate = jnp.concatenate([gate[:group], halves_added(gate[group:])], 0)
        up = jnp.concatenate([up[:group], halves_added(up[group:])], 0)
        hidden = gate / (1.0 + jnp.exp(-gate)) * up
        low = hidden[group:, : deep // 2]
        high = hidden[group:, deep // 2 :]
        narrow = jnp.where(half_rows(group, deep // 2) > 0.0, low, high)
        h_ref[lane, rows, :deep] = hidden[:group].astype(jnp.bfloat16)
        h_ref[lane, rows, deep:] = narrow.astype(jnp.bfloat16)

    def output_of(p):
        rows = group_rows(p)
        left_half = half_rows(group, deep // 2)
        total_a = None
        total_b = None
        for j in range(LANES):
            lhs = jnp.concatenate(
                [h_ref[j, rows, :deep], widened(h_ref[j, rows, deep:], left_half)], 0
            )
            z = jnp.dot(
                lhs, wd_ref[j * deep : (j + 1) * deep, :], preferred_element_type=jnp.float32
            )
            a = z[:group].astype(jnp.bfloat16).astype(jnp.float32)
            b = halves_added(z[group:]).astype(jnp.bfloat16).astype(jnp.float32)
            total_a = a if total_a is None else total_a + a
            total_b = b if total_b is None else total_b + b
        narrow = jnp.where(half_rows(group, half) > 0.0, total_b[:, :half], total_b[:, half:])
        y_ref[rows, :wide] = total_a.astype(jnp.bfloat16)
        y_ref[rows, wide:] = narrow.astype(jnp.bfloat16)

    def step(t, _):
        @pl.when(t < count)
        def _():
            @pl.when(t == own_group)
            def _():
                own_in.wait()

            def arrived(i, _):
                others(t * members + i, lambda index: go(index).wait_recv())
                return 0

            lax.fori_loop(0, members, arrived, 0)
            ring(t, 0).start()
            ring(t, 1).start()

        @pl.when((t >= 1) & (t < count + 1))
        def _():
            ring(t - 1, 0).wait_recv()
            passed(t - 1, 0).start()
            ring(t - 1, 1).wait_recv()
            passed(t - 1, 1).start()

        @pl.when((t >= 2) & (t < count + 2))
        def _():
            passed(t - 2, 0).wait_recv()
            passed(t - 2, 1).wait_recv()
            hidden_of(t - 2)
            for way in range(LANES - 1):
                hid(t - 2, way).start()

        @pl.when(t >= 3)
        def _():
            for way in range(LANES - 1):
                hid(t - 3, way).wait_recv()
            output_of(t - 3)

            @pl.when(t == own_group + 3)
            def _():
                own_out.start()

            def send_back(i, _):
                others((t - 3) * members + i, lambda index: back(index).start())
                return 0

            lax.fori_loop(0, members, send_back, 0)

        return 0

    lax.fori_loop(0, count + 3, step, 0)
    own_out.wait()

    def finish(index, _):
        def ended(index):
            go(index).wait_send()
            back(index).wait_send()
            back(index).wait_recv()

        others(index, ended)
        return 0

    lax.fori_loop(0, blocks, finish, 0)

    moe = None
    for k in range(2):

        def chosen(column, source):
            return jnp.dot(
                pick(column + k).astype(jnp.bfloat16), source, preferred_element_type=jnp.float32
            )

        expert_out = chosen(0, ret_ref[:, :wide]) + jnp.concatenate(
            [chosen(2, ret_ref[:, wide:]), chosen(4, ret_ref[:, wide:])], 1
        )
        term = table_ref[:, 6 + k : 7 + k] * expert_out
        moe = term if moe is None else moe + term
    mixed = deep_alpha * x1_ref[...].astype(jnp.float32) + moe
    lanes_of = (right, left, far)

    def s_go(way):
        return pltpu.make_async_remote_copy(
            src_ref=stat_ref.at[lane],
            dst_ref=stat_ref.at[lane],
            send_sem=s_send.at[way],
            recv_sem=s_recv.at[way],
            device_id={"sp": sp, "tp": lanes_of[way]},
            device_id_type=MESH,
        )

    own_tokens = tokens // LANES

    def m_go(way):
        rows = pl.ds(pl.multiple_of(lanes_of[way] * own_tokens, own_tokens), own_tokens)
        return pltpu.make_async_remote_copy(
            src_ref=mixed_ref.at[rows],
            dst_ref=final_ref.at[:, pl.ds(pl.multiple_of(lane * wide, wide), wide)],
            send_sem=m_send.at[way],
            recv_sem=m_recv.at[way],
            device_id={"sp": sp, "tp": lanes_of[way]},
            device_id_type=MESH,
        )

    gain = gain_ref[:, pl.ds(pl.multiple_of(lane * wide, wide), wide)]
    mixed_ref[...] = norm_over_lanes(mixed, gain, stat_ref, s_go, lane).astype(jnp.bfloat16)
    for way in range(LANES - 1):
        m_go(way).start()
    final_ref[:, pl.ds(pl.multiple_of(lane * wide, wide), wide)] = mixed_ref[
        pl.ds(pl.multiple_of(lane * own_tokens, own_tokens), own_tokens)
    ]
    for way in range(LANES - 1):
        s_go(way).wait_send()
        m_go(way).wait_recv()
        m_go(way).wait_send()

    def finish_group(p, _):
        for way in range(2):
            ring(p, way).wait_send()
            passed(p, way).wait_send()
        for way in range(LANES - 1):
            hid(p, way).wait_send()
        return 0

    lax.fori_loop(0, count, finish_group, 0)


def moe_layer(x_one, table, gain, w_gate, w_up, w_down):
    tokens, wide = x_one.shape
    rows, columns = Z_SIZE * X_SIZE * 2 * 8, wide * 3 // 2
    hidden = w_gate.shape[1]
    blocks = rows // 8
    vmem = pl.BlockSpec(memory_space=pltpu.VMEM)
    dma = pltpu.SemaphoreType.DMA
    return pl.pallas_call(
        moe_kernel,
        in_specs=[vmem] * 6,
        out_specs=vmem,
        out_shape=jax.ShapeDtypeStruct((tokens // LANES, wide * LANES), jnp.bfloat16),
        scratch_shapes=[
            pltpu.VMEM((rows, columns), jnp.bfloat16),
            pltpu.VMEM((rows, columns), jnp.bfloat16),
            pltpu.VMEM((tokens, wide), jnp.bfloat16),
            pltpu.VMEM((LANES, 8, tokens), jnp.float32),
            pltpu.VMEM((LANES, rows, columns), jnp.bfloat16),
            pltpu.VMEM((LANES, rows, hidden * 3 // 2), jnp.bfloat16),
            pltpu.VMEM((rows, columns), jnp.bfloat16),
            dma((blocks,)),
            dma((blocks,)),
            dma((GROUPS, 2)),
            dma((GROUPS, 2)),
            dma((GROUPS, 2)),
            dma((GROUPS, 2)),
            dma((GROUPS, LANES - 1)),
            dma((GROUPS, LANES - 1)),
            dma((blocks,)),
            dma((blocks,)),
            dma((LANES - 1,)),
            dma((LANES - 1,)),
            dma((LANES - 1,)),
            dma((LANES - 1,)),
        ],
        compiler_params=pltpu.CompilerParams(
            vmem_limit_bytes=VMEM_LIMIT, collective_id=1, has_side_effects=True
        ),
        cost_estimate=pl.CostEstimate(
            flops=12 * LANES * rows * 1024 * hidden,
            bytes_accessed=200_000_000,
            transcendentals=0,
        ),
        name="experts",
    )(x_one, table, gain, w_gate, w_up, w_down)


def per_device(
    resid,
    queries,
    keys,
    values,
    q_gain,
    key_norm_gain,
    out_weight,
    norm1_gain,
    norm2_gain,
    expert_ids,
    group_weight,
    expert_weight,
    gate_proj,
    up_proj,
    down_proj,
):
    tokens = queries.shape[0]
    width = q_gain.shape[0]
    heads = queries.shape[1] // width
    lanes = lax.axis_size("tp")
    sp_count = lax.axis_size("sp")
    lane = lax.axis_index("tp")
    own = tokens // lanes
    model_width = resid.shape[1]
    part = model_width // lanes

    positions = lax.axis_index("sp") * tokens + jnp.arange(tokens, dtype=jnp.int32)
    rotated_keys = apply_rotary_heads(keys.reshape(tokens, 1, width), key_norm_gain, positions)
    both = jnp.concatenate([rotated_keys.reshape(tokens, width), values], 1)
    gates_own = (
        group_weight[:, None] * expert_weight / jnp.sum(expert_weight, -1, keepdims=True)
    )
    top = expert_ids.shape[1]
    sp = lax.axis_index("sp")
    flat = expert_ids.reshape(-1)
    one_hot = (flat[:, None] == jnp.arange(sp_count, dtype=jnp.int32)).astype(jnp.int32)
    earlier = jnp.cumsum(one_hot, 0) - one_hot
    rank = jnp.sum(earlier * one_hot, 1)
    dz = (flat // (2 * X_SIZE) - sp // (2 * X_SIZE)) % Z_SIZE
    dx = (flat // 2 - sp // 2) % X_SIZE
    dc = (flat - sp) % 2
    near = jnp.where(dz <= Z_SIZE // 2, 2 * dz - 2, 2 * (Z_SIZE - dz) - 1)
    near = jnp.where(dz == 0, Z_SIZE - 1, near)
    target = ((near * X_SIZE + dx) * 2 + dc) * 8
    place = lane * CAP + rank
    row_a = jnp.where(place < 8, target + place, -1)
    row_b = jnp.where(place < 8, -1, target + place - 8)
    row_c = jnp.where(place < 8, -1, target + place - 4)
    info = jnp.concatenate(
        [v.reshape(own, top).astype(jnp.float32) for v in (row_a, row_b, row_c)]
        + [gates_own, jnp.zeros((own, 128 - 4 * top), jnp.float32)],
        1,
    )

    q_rot = apply_rotary_heads(queries.reshape(tokens, heads, width), q_gain, positions)
    factor = np.float32(np.log2(np.e) * width**-0.5)
    scaled = q_rot.astype(jnp.float32) * factor
    coarse = lax.reduce_precision(scaled, 8, 7)
    fine = (scaled - coarse).astype(jnp.bfloat16)
    pair = jnp.concatenate([coarse.astype(jnp.bfloat16), fine], -1)
    q_t = pair.transpose(2, 1, 0).reshape(2 * width, heads * tokens)
    x_one, down_slice, table = front(
        q_t, both, out_weight, down_proj[0], resid, info, norm1_gain[None]
    )
    return moe_layer(
        x_one,
        table.reshape(tokens, -1),
        norm2_gain[None],
        gate_proj[0],
        up_proj[0],
        down_slice.reshape(-1, part),
    )


def solution(mesh):
    in_specs = (
        P(("sp", "tp"), None),
        P("sp", "tp"),
        P("sp", "tp"),
        P("sp", "tp"),
        P(),
        P(),
        P("tp", None),
        P(),
        P(),
        P(("sp", "tp"), None),
        P(("sp", "tp")),
        P(("sp", "tp"), None),
        P("sp", None, "tp"),
        P("sp", None, "tp"),
        P("sp", "tp", None),
    )
    out_specs = P(("sp", "tp"), None)
    return jax.shard_map(
        per_device, mesh=mesh, in_specs=in_specs, out_specs=out_specs, check_vma=False
    )
```

```python
import jax
import jax.numpy as jnp
import numpy as np
from jax import lax
from jax.experimental import pallas as pl
from jax.experimental.pallas import tpu as pltpu
from jax.sharding import PartitionSpec as P

GRID_W = 64
CAP = 3
QUERY_TILE = 512

deep_alpha = 2.0**0.5
rope_theta = 10000.0
VMEM_LIMIT = 60 * 1024 * 1024
MESH = pl.DeviceIdType.MESH
Z_SIZE = 8
X_SIZE = 4
LANES = 4
GROUPS = 16


def apply_rotary_heads(block, gain, grid_positions):
    values32 = block.astype(jnp.float32)
    normed = values32 * lax.rsqrt(jnp.mean(values32 * values32, -1, keepdims=True) + 1e-06) * gain
    half = normed.shape[-1] // 2
    inv_freq = rope_theta ** (-jnp.arange(0, half, 2, dtype=jnp.float32) / half)
    grid_row = (grid_positions // GRID_W).astype(jnp.float32)
    grid_col = (grid_positions % GRID_W).astype(jnp.float32)
    angle = jnp.concatenate([grid_row[:, None] * inv_freq, grid_col[:, None] * inv_freq], -1)[
        :, None, :
    ]
    cosine = jnp.cos(angle)
    sine = jnp.sin(angle)
    first = normed[..., :half]
    second = normed[..., half:]
    turned = jnp.concatenate([first * cosine - second * sine, first * sine + second * cosine], -1)
    return turned.astype(jnp.bfloat16)


def front_kernel(
    qt_ref,
    own_ref,
    w_ref,
    wd_ref,
    resid_ref,
    info_ref,
    gain_ref,
    x_ref,
    down_ref,
    table_ref,
    kv_ref,
    m_ref,
    l_ref,
    acc_ref,
    attn_ref,
    out_ref,
    res_ref,
    stat_ref,
    tx,
    rx_full,
    rx_half,
    rx_core,
    load_sem,
    w_send,
    w_recv,
    w_pair_send,
    w_pair_recv,
    d_send,
    d_recv,
    r_send,
    r_recv,
    i_send,
    i_recv,
    a_send,
    a_recv,
    s_send,
    s_recv,
):
    sp = lax.axis_index("sp")
    lane = lax.axis_index("tp")
    core = lax.rem(sp, 2)
    x_at = lax.rem(sp // 2, X_SIZE)
    z_at = sp // (2 * X_SIZE)
    partner = sp + 1 - 2 * core
    block = own_ref.shape[0]
    width = own_ref.shape[1] // 2
    rows = qt_ref.shape[1]
    heads = rows // block
    wide = x_ref.shape[1]
    lane_rows = res_ref.shape[1]
    depth = out_ref.shape[1]
    lanes_of = [lax.rem(lane + 1, LANES), lax.rem(lane + LANES - 1, LANES), lax.rem(lane + 2, LANES)]
    froms = [lanes_of[1], lanes_of[0], lanes_of[2]]

    def sp_of(z, x, c):
        return (lax.rem(z + 2 * Z_SIZE, Z_SIZE) * X_SIZE + lax.rem(x + 2 * X_SIZE, X_SIZE)) * 2 + c

    ways = (
        sp_of(z_at + 1, x_at, core),
        sp_of(z_at - 1, x_at, core),
        sp_of(z_at, x_at + 1, core),
        sp_of(z_at, x_at - 1, core),
        partner,
    )
    barrier = pltpu.get_barrier_semaphore()
    for way in range(5):
        pl.semaphore_signal(
            barrier, inc=1, device_id={"sp": ways[way], "tp": lane}, device_id_type=MESH
        )
    for other in lanes_of:
        pl.semaphore_signal(
            barrier, inc=1, device_id={"sp": sp, "tp": other}, device_id_type=MESH
        )

    own_copy = pltpu.make_async_copy(own_ref, kv_ref.at[core, z_at, x_at], load_sem.at[0])
    w_copy = pltpu.make_async_copy(
        w_ref.at[:, pl.ds(pl.multiple_of(lane * wide, wide), wide)], out_ref.at[lane], load_sem.at[1]
    )
    d_copy = pltpu.make_async_copy(
        wd_ref.at[:, pl.ds(pl.multiple_of(lane * wide, wide), wide)], down_ref.at[lane], load_sem.at[2]
    )
    r_copy = pltpu.make_async_copy(
        resid_ref.at[:, pl.ds(pl.multiple_of(lane * wide, wide), wide)], res_ref.at[lane], load_sem.at[3]
    )
    i_copy = pltpu.make_async_copy(info_ref, table_ref.at[lane], load_sem.at[4])
    own_copy.start()

    def to_lane(src, dst, send, recv, way):
        return pltpu.make_async_remote_copy(
            src_ref=src,
            dst_ref=dst,
            send_sem=send.at[way],
            recv_sem=recv.at[way],
            device_id={"sp": sp, "tp": lanes_of[way]},
            device_id_type=MESH,
        )

    def columns(way):
        return pl.ds(pl.multiple_of(lanes_of[way] * wide, wide), wide)

    part_rows = depth // 2
    half = pl.ds(pl.multiple_of(core * part_rows, part_rows), part_rows)

    def w_go(way):
        return to_lane(w_ref.at[half, columns(way)], out_ref.at[lane, half], w_send, w_recv, way)

    def w_pair(way):
        return pltpu.make_async_remote_copy(
            src_ref=out_ref.at[froms[way], half],
            dst_ref=out_ref.at[froms[way], half],
            send_sem=w_pair_send.at[way],
            recv_sem=w_pair_recv.at[way],
            device_id={"sp": partner, "tp": lane},
            device_id_type=MESH,
        )

    def d_go(way):
        return to_lane(wd_ref.at[:, columns(way)], down_ref.at[lane], d_send, d_recv, way)

    def r_go(way):
        return to_lane(resid_ref.at[:, columns(way)], res_ref.at[lane], r_send, r_recv, way)

    def i_go(way):
        return to_lane(info_ref, table_ref.at[lane], i_send, i_recv, way)

    def a_go(way):
        return to_lane(attn_ref.at[lane], attn_ref.at[lane], a_send, a_recv, way)

    def s_go(way):
        return to_lane(stat_ref.at[lane], stat_ref.at[lane], s_send, s_recv, way)

    def send(cls, zz, xx, way, piece=None):
        if piece is None:
            at = kv_ref.at[cls, zz, xx]
            recv = rx_core.at[zz, xx] if way == 4 else rx_full.at[zz, xx]
        else:
            at = kv_ref.at[cls, zz, xx, pl.ds(piece * (block // 2), block // 2)]
            recv = rx_half.at[zz, xx, piece]
        return pltpu.make_async_remote_copy(
            src_ref=at,
            dst_ref=at,
            send_sem=tx.at[zz, xx, way],
            recv_sem=recv,
            device_id={"sp": ways[way], "tp": lane},
            device_id_type=MESH,
        )

    def wait_block(zz, xx, halves):
        if halves:
            send(core, zz, xx, 0, 0).wait_recv()
            send(core, zz, xx, 0, 1).wait_recv()
        else:
            send(core, zz, xx, 0).wait_recv()

    def z_of(d):
        return lax.rem(z_at + d + Z_SIZE, Z_SIZE)

    x_order = [
        x_at,
        lax.rem(x_at + X_SIZE - 1, X_SIZE),
        lax.rem(x_at + 1, X_SIZE),
        lax.rem(x_at + 2, X_SIZE),
    ]

    def along_x(zz, s, act):
        if s == 0:
            act(send(core, zz, x_order[0], 2))
            act(send(core, zz, x_order[0], 3))
        elif s == 1:
            act(send(core, zz, x_order[1], 2, 0))
        elif s == 2:
            act(send(core, zz, x_order[2], 3, 1))

    def along_z(h, xx, side, act):
        zz = z_of(-h if side == 0 else h)

        @pl.when(h < 3)
        def _():
            act(send(core, zz, xx, side))

        @pl.when(h == 3)
        def _():
            act(send(core, zz, xx, side, side))

    def first(s, act, wait):
        xx = x_order[s]
        if wait and s > 0:
            wait_block(z_at, xx, s == 3)
        along_x(z_at, s, act)

        if s == 0:
            act(send(core, z_at, xx, 0))
            act(send(core, z_at, xx, 1))
        else:

            @pl.when(core == 0)
            def _():
                act(send(core, z_at, xx, 0))
                act(send(core, z_at, xx, 1))

        act(send(core, z_at, xx, 4))

    def later(h, s, act, wait):
        xx = x_order[s]

        @pl.when(core == 0)
        def _():
            @pl.when(h < 4)
            def _():
                for side in range(2):
                    zz = z_of(-h if side == 0 else h)
                    if wait:
                        wait_block(zz, xx, False)
                    along_z(h, xx, side, act)
                    act(send(core, zz, xx, 4))

            @pl.when(h == 4)
            def _():
                zz = z_of(4)
                if wait:
                    wait_block(zz, xx, True)
                act(send(core, zz, xx, 4))

        @pl.when(core == 1)
        def _():
            if s == 0:

                @pl.when(h < 4)
                def _():
                    ahead(h + 1, act, wait)
            else:

                @pl.when(h < 4)
                def _():
                    for side in range(2):
                        zz = z_of(-h if side == 0 else h)
                        if wait:
                            wait_block(zz, xx, s == 3)
                        along_x(zz, s, act)
                        act(send(core, zz, xx, 4))

                @pl.when(h == 4)
                def _():
                    zz = z_of(4)
                    if wait:
                        wait_block(zz, xx, s == 3)
                    along_x(zz, s, act)
                    act(send(core, zz, xx, 4))

    def ahead(h, act, wait):
        @pl.when(h < 4)
        def _():
            for side in range(2):
                zz = z_of(-h if side == 0 else h)
                if wait:
                    wait_block(zz, x_at, False)
                along_z(h, x_at, side, act)
                along_x(zz, 0, act)
                act(send(core, zz, x_at, 4))

        @pl.when(h == 4)
        def _():
            zz = z_of(4)
            if wait:
                wait_block(zz, x_at, True)
            along_x(zz, 0, act)
            act(send(core, zz, x_at, 4))

    def start(copy):
        copy.start()

    def ended(copy):
        copy.wait_send()

    m_ref[...] = jnp.full_like(m_ref, -1e30)
    l_ref[...] = jnp.zeros_like(l_ref)
    acc_ref[...] = jnp.zeros_like(acc_ref)
    own_copy.wait()
    pl.semaphore_wait(barrier, 5 + LANES - 1)
    first(0, start, True)
    for way in range(LANES - 1):
        i_go(way).start()
    for way in range(LANES - 1):
        w_go(way).start()
    for way in range(LANES - 1):
        r_go(way).start()
    for way in range(LANES - 1):
        d_go(way).start()
    w_copy.start()
    r_copy.start()
    d_copy.start()
    i_copy.start()

    @pl.when(core == 1)
    def _():
        ahead(1, start, True)

    for s in range(1, 4):
        first(s, start, True)

    tile = min(QUERY_TILE, rows)
    keys = X_SIZE * block

    def attend(cls, zz):
        both = kv_ref[cls, zz].reshape(keys, 2 * width)
        k = both[:, :width]
        k_twice = jnp.concatenate([k, k], 1)
        v_t = both[:, width:].T

        def scores(t):
            return jnp.dot(
                k_twice, qt_ref[:, t * tile : (t + 1) * tile], preferred_element_type=jnp.float32
            )

        s = scores(0)
        for t in range(rows // tile):
            following = scores(t + 1) if t + 1 < rows // tile else None
            at = slice(t * tile, (t + 1) * tile)
            m_old = m_ref[:, at]
            m_new = jnp.maximum(m_old, jnp.max(s, 0, keepdims=True))
            shrink = jnp.exp2(m_old - m_new)
            p = jnp.exp2(s - m_new)
            l_ref[:, at] = l_ref[:, at] * shrink + jnp.sum(p, 0, keepdims=True)
            m_ref[:, at] = m_new
            pv = jnp.dot(v_t, p.astype(jnp.bfloat16), preferred_element_type=jnp.float32)
            acc_ref[:, at] = acc_ref[:, at] * shrink + pv
            s = following

    def slot(i, _):
        dist = jnp.where(i < 2, 0, (i - 2) // 4 + 1)
        turn = lax.rem(i + 2, 4)
        ours = jnp.where((dist == 0) | (dist == 4), lax.rem(i, 2) == 0, turn < 2)
        side = jnp.where((dist == 0) | (dist == 4), 1, lax.rem(i, 2))
        zz = z_of(jnp.where(side == 0, -dist, dist))
        cls = jnp.where(ours, core, 1 - core)

        @pl.when(cls != core)
        def _():
            for xx in range(X_SIZE):
                pltpu.make_async_remote_copy(
                    src_ref=kv_ref.at[cls, zz, xx],
                    dst_ref=kv_ref.at[cls, zz, xx],
                    send_sem=tx.at[zz, xx, 4],
                    recv_sem=rx_core.at[zz, xx],
                    device_id={"sp": partner, "tp": lane},
                    device_id_type=MESH,
                ).wait_recv()

        attend(cls, zz)
        for s in range(4):

            @pl.when(((i < 2) & (s // 2 == i)) | ((i >= 2) & (i < 14) & (turn == s)))
            def _(s=s):
                later(dist + 1, s, start, True)

        @pl.when(i == 12)
        def _():
            for way in range(LANES - 1):
                w_go(way).wait_recv()
                w_pair(way).start()

        return 0

    lax.fori_loop(0, 16, slot, 0)

    for h in range(heads):
        at = slice(h * block, (h + 1) * block)
        out = acc_ref[:, at] / l_ref[:, at]
        attn_ref[lane, :, h * width : (h + 1) * width] = out.T.astype(jnp.bfloat16)
    for way in (2, 0, 1):
        a_go(way).start()
    w_copy.wait()
    for way in range(LANES - 1):
        w_pair(way).wait_recv()
    total = jnp.dot(attn_ref[lane], out_ref[lane], preferred_element_type=jnp.float32)
    for way in range(LANES - 1):
        a_go(way).wait_recv()
        total = total + jnp.dot(
            attn_ref[froms[way]], out_ref[froms[way]], preferred_element_type=jnp.float32
        )
    r_copy.wait()
    for way in range(LANES - 1):
        r_go(way).wait_recv()
    summed = deep_alpha * res_ref[...].reshape(LANES * lane_rows, wide).astype(jnp.float32)
    summed = summed + total.astype(jnp.bfloat16).astype(jnp.float32)
    gain = gain_ref[:, pl.ds(pl.multiple_of(lane * wide, wide), wide)]
    normed = norm_over_lanes(summed, gain, stat_ref, s_go, lane)
    x_ref[...] = normed.astype(jnp.bfloat16)

    i_copy.wait()
    d_copy.wait()
    for way in range(LANES - 1):
        i_go(way).wait_recv()
        d_go(way).wait_recv()
        w_go(way).wait_send()
        w_pair(way).wait_send()
        r_go(way).wait_send()
        i_go(way).wait_send()
        d_go(way).wait_send()
        a_go(way).wait_send()
        s_go(way).wait_send()
    for s in range(4):
        first(s, ended, False)

    @pl.when(core == 1)
    def _():
        ahead(1, ended, False)

    def finish(h, _):
        for s in range(4):
            later(h, s, ended, False)
        return 0

    lax.fori_loop(1, 5, finish, 0)


def norm_over_lanes(z, gain, stat_ref, s_go, lane):
    rows, wide = z.shape
    mean = jnp.sum(z, 1, keepdims=True) * (1.0 / wide)
    centre = z - mean
    m2 = jnp.sum(centre * centre, 1, keepdims=True)
    column = lax.broadcasted_iota(jnp.int32, (rows, 128), 1)
    both = jnp.where(column == 0, mean, m2)
    stat_ref[lane] = both.T[:8]
    for way in range(LANES - 1):
        s_go(way).start()
    for way in range(LANES - 1):
        s_go(way).wait_recv()
    means = [stat_ref[j][0:1] for j in range(LANES)]
    m2s = [stat_ref[j][1:2] for j in range(LANES)]
    full = (means[0] + means[1] + means[2] + means[3]) * (1.0 / LANES)
    away = sum((v - full) * (v - full) for v in means)
    spread = (m2s[0] + m2s[1] + m2s[2] + m2s[3] + wide * away) * (1.0 / (wide * LANES))
    scale = lax.rsqrt(spread + 1e-06)
    row = lax.broadcasted_iota(jnp.int32, (128, rows), 0)
    packed = jnp.where(row == 0, full, scale).T
    return (z - packed[:, 0:1]) * packed[:, 1:2] * gain


def front(q_t, keys_values, out_weight, down_proj, resid, info, gain):
    tokens, pair = keys_values.shape
    width = pair // 2
    rows = q_t.shape[1]
    depth, model = out_weight.shape
    wide = model // LANES
    vmem = pl.BlockSpec(memory_space=pltpu.VMEM)
    hbm = pl.BlockSpec(memory_space=pltpu.HBM)
    dma = pltpu.SemaphoreType.DMA
    others = LANES - 1
    return pl.pallas_call(
        front_kernel,
        in_specs=[vmem, vmem, hbm, hbm, hbm, vmem, vmem],
        out_specs=[vmem, vmem, vmem],
        out_shape=[
            jax.ShapeDtypeStruct((tokens, wide), jnp.bfloat16),
            jax.ShapeDtypeStruct((LANES, down_proj.shape[0], wide), jnp.bfloat16),
            jax.ShapeDtypeStruct((LANES, *info.shape), jnp.float32),
        ],
        scratch_shapes=[
            pltpu.VMEM((2, Z_SIZE, X_SIZE, tokens, pair), jnp.bfloat16),
            pltpu.VMEM((1, rows), jnp.float32),
            pltpu.VMEM((1, rows), jnp.float32),
            pltpu.VMEM((width, rows), jnp.float32),
            pltpu.VMEM((LANES, tokens, depth), jnp.bfloat16),
            pltpu.VMEM((LANES, depth, wide), jnp.bfloat16),
            pltpu.VMEM((LANES, resid.shape[0], wide), jnp.bfloat16),
            pltpu.VMEM((LANES, 8, tokens), jnp.float32),
            dma((Z_SIZE, X_SIZE, 5)),
            dma((Z_SIZE, X_SIZE)),
            dma((Z_SIZE, X_SIZE, 2)),
            dma((Z_SIZE, X_SIZE)),
            dma((5,)),
        ]
        + [dma((others,))] * 14,
        compiler_params=pltpu.CompilerParams(
            vmem_limit_bytes=VMEM_LIMIT, collective_id=2, has_side_effects=True
        ),
        cost_estimate=pl.CostEstimate(
            flops=20_000_000_000, bytes_accessed=100_000_000, transcendentals=rows * 16384
        ),
        name="front",
    )(q_t, keys_values, out_weight, down_proj, resid, info, gain)


def half_rows(rows, columns):
    row = lax.broadcasted_iota(jnp.int32, (rows, columns), 0)
    return ((row % 8) < 4).astype(jnp.float32)


def widened(block, left):
    value = block.astype(jnp.float32)
    first = value * left
    return jnp.concatenate([first, value - first], 1).astype(jnp.bfloat16)


def halves_added(value):
    rows, columns = value.shape
    parts = value.reshape(rows // 8, 8, columns)
    return (parts + pltpu.roll(parts, 4, 1)).reshape(rows, columns)


def moe_kernel(
    x1_ref,
    table_ref,
    gain_ref,
    wg_ref,
    wu_ref,
    wd_ref,
    final_ref,
    out_ref,
    ret_ref,
    mixed_ref,
    stat_ref,
    x_ref,
    h_ref,
    y_ref,
    go_send,
    go_recv,
    ring_send,
    ring_recv,
    pass_send,
    pass_recv,
    hid_send,
    hid_recv,
    back_send,
    back_recv,
    s_send,
    s_recv,
    m_send,
    m_recv,
):
    sp = lax.axis_index("sp")
    lane = lax.axis_index("tp")
    core = lax.rem(sp, 2)
    x_at = lax.rem(sp // 2, X_SIZE)
    z_at = sp // (2 * X_SIZE)
    right = lax.rem(lane + 1, LANES)
    left = lax.rem(lane + LANES - 1, LANES)
    far = lax.rem(lane + 2, LANES)
    wide = wd_ref.shape[1]
    half = wide // 2
    deep = wd_ref.shape[0] // LANES
    peers = X_SIZE * 2
    blocks = Z_SIZE * peers
    count = GROUPS
    members = blocks // count
    group = 8 * members

    def z_offset(p):
        away = jnp.where(lax.rem(p, 2) == 0, p // 2 + 1, Z_SIZE - (p + 1) // 2)
        return jnp.where(p == Z_SIZE - 1, 0, away)

    def peer(index, sign):
        p = index // peers
        dx = lax.rem(index, peers) // 2
        dc = lax.rem(index, 2)
        z = lax.rem(z_at + sign * z_offset(p) + Z_SIZE, Z_SIZE)
        x = lax.rem(x_at + sign * dx + X_SIZE, X_SIZE)
        c = lax.rem(core + dc, 2)
        return (z * X_SIZE + x) * 2 + c

    def rows_of(index):
        return pl.ds(pl.multiple_of(index * 8, 8), 8)

    def group_rows(p):
        return pl.ds(pl.multiple_of(p * group, group), group)

    barrier = pltpu.get_barrier_semaphore()

    own_index = (Z_SIZE - 1) * peers
    own_group = own_index // members

    def others(index, what):
        @pl.when(index != own_index)
        def _():
            what(index)

    def greet(index, _):
        def signal(index):
            pl.semaphore_signal(
                barrier, inc=1, device_id={"sp": peer(index, 1), "tp": lane}, device_id_type=MESH
            )

        others(index, signal)
        return 0

    lax.fori_loop(0, blocks, greet, 0)
    for other in (left, right, far):
        pl.semaphore_signal(
            barrier, inc=1, device_id={"sp": sp, "tp": other}, device_id_type=MESH
        )
    tokens = x1_ref.shape[0]
    spots = lax.broadcasted_iota(jnp.int32, (tokens, blocks * 8), 1).astype(jnp.float32)

    def pick(column):
        return (spots == table_ref[:, column : column + 1]).astype(jnp.float32)

    def placed(first, second, source):
        return lax.dot_general(
            (pick(first) + pick(second)).astype(jnp.bfloat16),
            source,
            (((0,), (0,)), ((), ())),
            preferred_element_type=jnp.float32,
        )

    x1 = x1_ref[...]
    out_ref[:, :wide] = placed(0, 1, x1).astype(jnp.bfloat16)
    out_ref[:, wide:] = (placed(2, 3, x1[:, :half]) + placed(4, 5, x1[:, half:])).astype(
        jnp.bfloat16
    )
    pl.semaphore_wait(barrier, blocks - 1 + LANES - 1)

    def go(index):
        return pltpu.make_async_remote_copy(
            src_ref=out_ref.at[rows_of(index)],
            dst_ref=x_ref.at[lane, rows_of(index)],
            send_sem=go_send.at[index],
            recv_sem=go_recv.at[index],
            device_id={"sp": peer(index, 1), "tp": lane},
            device_id_type=MESH,
        )

    def back(index):
        return pltpu.make_async_remote_copy(
            src_ref=y_ref.at[rows_of(index)],
            dst_ref=ret_ref.at[rows_of(index)],
            send_sem=back_send.at[index],
            recv_sem=back_recv.at[index],
            device_id={"sp": peer(index, -1), "tp": lane},
            device_id_type=MESH,
        )

    def ring(p, way):
        return pltpu.make_async_remote_copy(
            src_ref=x_ref.at[lane, group_rows(p)],
            dst_ref=x_ref.at[lane, group_rows(p)],
            send_sem=ring_send.at[p, way],
            recv_sem=ring_recv.at[p, way],
            device_id={"sp": sp, "tp": right if way == 0 else left},
            device_id_type=MESH,
        )

    def passed(p, way):
        owner = left if way == 0 else right
        rows = pl.ds(pl.multiple_of(p * group + way * (group // 2), group // 2), group // 2)
        return pltpu.make_async_remote_copy(
            src_ref=x_ref.at[owner, rows],
            dst_ref=x_ref.at[owner, rows],
            send_sem=pass_send.at[p, way],
            recv_sem=pass_recv.at[p, way],
            device_id={"sp": sp, "tp": right if way == 0 else left},
            device_id_type=MESH,
        )

    def hid(p, way):
        return pltpu.make_async_remote_copy(
            src_ref=h_ref.at[lane, group_rows(p)],
            dst_ref=h_ref.at[lane, group_rows(p)],
            send_sem=hid_send.at[p, way],
            recv_sem=hid_recv.at[p, way],
            device_id={"sp": sp, "tp": (right, left, far)[way]},
            device_id_type=MESH,
        )

    own_rows = pl.ds(own_index * 8, 8)
    own_in = pltpu.make_async_copy(
        out_ref.at[own_rows], x_ref.at[lane, own_rows], go_recv.at[own_index]
    )
    own_out = pltpu.make_async_copy(
        y_ref.at[own_rows], ret_ref.at[own_rows], back_recv.at[own_index]
    )
    own_in.start()

    def send_one(index, _):
        others(index, lambda i: go(i).start())
        return 0

    lax.fori_loop(0, blocks, send_one, 0)

    def hidden_of(p):
        rows = group_rows(p)
        left_half = half_rows(group, half)
        gate = None
        up = None
        for j in range(LANES):
            lhs = jnp.concatenate(
                [x_ref[j, rows, :wide], widened(x_ref[j, rows, wide:], left_half)], 0
            )
            g = jnp.dot(
                lhs, wg_ref[j * wide : (j + 1) * wide, :], preferred_element_type=jnp.float32
            )
            u = jnp.dot(
                lhs, wu_ref[j * wide : (j + 1) * wide, :], preferred_element_type=jnp.float32
            )
            gate = g if gate is None else gate + g
            up = u if up is None else up + u
        gate = jnp.concatenate([gate[:group], halves_added(gate[group:])], 0)
        up = jnp.concatenate([up[:group], halves_added(up[group:])], 0)
        hidden = gate / (1.0 + jnp.exp(-gate)) * up
        low = hidden[group:, : deep // 2]
        high = hidden[group:, deep // 2 :]
        narrow = jnp.where(half_rows(group, deep // 2) > 0.0, low, high)
        h_ref[lane, rows, :deep] = hidden[:group].astype(jnp.bfloat16)
        h_ref[lane, rows, deep:] = narrow.astype(jnp.bfloat16)

    def output_of(p):
        rows = group_rows(p)
        left_half = half_rows(group, deep // 2)
        total_a = None
        total_b = None
        for j in range(LANES):
            lhs = jnp.concatenate(
                [h_ref[j, rows, :deep], widened(h_ref[j, rows, deep:], left_half)], 0
            )
            z = jnp.dot(
                lhs, wd_ref[j * deep : (j + 1) * deep, :], preferred_element_type=jnp.float32
            )
            a = z[:group].astype(jnp.bfloat16).astype(jnp.float32)
            b = halves_added(z[group:]).astype(jnp.bfloat16).astype(jnp.float32)
            total_a = a if total_a is None else total_a + a
            total_b = b if total_b is None else total_b + b
        narrow = jnp.where(half_rows(group, half) > 0.0, total_b[:, :half], total_b[:, half:])
        y_ref[rows, :wide] = total_a.astype(jnp.bfloat16)
        y_ref[rows, wide:] = narrow.astype(jnp.bfloat16)

    def step(t, _):
        @pl.when(t < count)
        def _():
            @pl.when(t == own_group)
            def _():
                own_in.wait()

            def arrived(i, _):
                others(t * members + i, lambda index: go(index).wait_recv())
                return 0

            lax.fori_loop(0, members, arrived, 0)
            ring(t, 0).start()
            ring(t, 1).start()

        @pl.when((t >= 1) & (t < count + 1))
        def _():
            ring(t - 1, 0).wait_recv()
            passed(t - 1, 0).start()
            ring(t - 1, 1).wait_recv()
            passed(t - 1, 1).start()

        @pl.when((t >= 2) & (t < count + 2))
        def _():
            passed(t - 2, 0).wait_recv()
            passed(t - 2, 1).wait_recv()
            hidden_of(t - 2)
            for way in (2, 0, 1):
                hid(t - 2, way).start()

        @pl.when(t >= 3)
        def _():
            for way in range(LANES - 1):
                hid(t - 3, way).wait_recv()
            output_of(t - 3)

            @pl.when(t == own_group + 3)
            def _():
                own_out.start()

            def send_back(i, _):
                others((t - 3) * members + i, lambda index: back(index).start())
                return 0

            lax.fori_loop(0, members, send_back, 0)

        return 0

    lax.fori_loop(0, count + 3, step, 0)
    own_out.wait()

    def finish(index, _):
        def ended(index):
            go(index).wait_send()
            back(index).wait_send()
            back(index).wait_recv()

        others(index, ended)
        return 0

    lax.fori_loop(0, blocks, finish, 0)

    moe = None
    for k in range(2):

        def chosen(column, source):
            return jnp.dot(
                pick(column + k).astype(jnp.bfloat16), source, preferred_element_type=jnp.float32
            )

        expert_out = chosen(0, ret_ref[:, :wide]) + jnp.concatenate(
            [chosen(2, ret_ref[:, wide:]), chosen(4, ret_ref[:, wide:])], 1
        )
        term = table_ref[:, 6 + k : 7 + k] * expert_out
        moe = term if moe is None else moe + term
    mixed = deep_alpha * x1_ref[...].astype(jnp.float32) + moe
    lanes_of = (right, left, far)

    def s_go(way):
        return pltpu.make_async_remote_copy(
            src_ref=stat_ref.at[lane],
            dst_ref=stat_ref.at[lane],
            send_sem=s_send.at[way],
            recv_sem=s_recv.at[way],
            device_id={"sp": sp, "tp": lanes_of[way]},
            device_id_type=MESH,
        )

    own_tokens = tokens // LANES

    def m_go(way):
        rows = pl.ds(pl.multiple_of(lanes_of[way] * own_tokens, own_tokens), own_tokens)
        return pltpu.make_async_remote_copy(
            src_ref=mixed_ref.at[rows],
            dst_ref=final_ref.at[:, pl.ds(pl.multiple_of(lane * wide, wide), wide)],
            send_sem=m_send.at[way],
            recv_sem=m_recv.at[way],
            device_id={"sp": sp, "tp": lanes_of[way]},
            device_id_type=MESH,
        )

    gain = gain_ref[:, pl.ds(pl.multiple_of(lane * wide, wide), wide)]
    mixed_ref[...] = norm_over_lanes(mixed, gain, stat_ref, s_go, lane).astype(jnp.bfloat16)
    for way in (2, 0, 1):
        m_go(way).start()
    final_ref[:, pl.ds(pl.multiple_of(lane * wide, wide), wide)] = mixed_ref[
        pl.ds(pl.multiple_of(lane * own_tokens, own_tokens), own_tokens)
    ]
    for way in range(LANES - 1):
        s_go(way).wait_send()
        m_go(way).wait_recv()
        m_go(way).wait_send()

    def finish_group(p, _):
        for way in range(2):
            ring(p, way).wait_send()
            passed(p, way).wait_send()
        for way in range(LANES - 1):
            hid(p, way).wait_send()
        return 0

    lax.fori_loop(0, count, finish_group, 0)


def moe_layer(x_one, table, gain, w_gate, w_up, w_down):
    tokens, wide = x_one.shape
    rows, columns = Z_SIZE * X_SIZE * 2 * 8, wide * 3 // 2
    hidden = w_gate.shape[1]
    blocks = rows // 8
    vmem = pl.BlockSpec(memory_space=pltpu.VMEM)
    dma = pltpu.SemaphoreType.DMA
    return pl.pallas_call(
        moe_kernel,
        in_specs=[vmem] * 6,
        out_specs=vmem,
        out_shape=jax.ShapeDtypeStruct((tokens // LANES, wide * LANES), jnp.bfloat16),
        scratch_shapes=[
            pltpu.VMEM((rows, columns), jnp.bfloat16),
            pltpu.VMEM((rows, columns), jnp.bfloat16),
            pltpu.VMEM((tokens, wide), jnp.bfloat16),
            pltpu.VMEM((LANES, 8, tokens), jnp.float32),
            pltpu.VMEM((LANES, rows, columns), jnp.bfloat16),
            pltpu.VMEM((LANES, rows, hidden * 3 // 2), jnp.bfloat16),
            pltpu.VMEM((rows, columns), jnp.bfloat16),
            dma((blocks,)),
            dma((blocks,)),
            dma((GROUPS, 2)),
            dma((GROUPS, 2)),
            dma((GROUPS, 2)),
            dma((GROUPS, 2)),
            dma((GROUPS, LANES - 1)),
            dma((GROUPS, LANES - 1)),
            dma((blocks,)),
            dma((blocks,)),
            dma((LANES - 1,)),
            dma((LANES - 1,)),
            dma((LANES - 1,)),
            dma((LANES - 1,)),
        ],
        compiler_params=pltpu.CompilerParams(
            vmem_limit_bytes=VMEM_LIMIT, collective_id=1, has_side_effects=True
        ),
        cost_estimate=pl.CostEstimate(
            flops=12 * LANES * rows * 1024 * hidden,
            bytes_accessed=200_000_000,
            transcendentals=0,
        ),
        name="experts",
    )(x_one, table, gain, w_gate, w_up, w_down)


def per_device(
    resid,
    queries,
    keys,
    values,
    q_gain,
    key_norm_gain,
    out_weight,
    norm1_gain,
    norm2_gain,
    expert_ids,
    group_weight,
    expert_weight,
    gate_proj,
    up_proj,
    down_proj,
):
    tokens = queries.shape[0]
    width = q_gain.shape[0]
    heads = queries.shape[1] // width
    lanes = lax.axis_size("tp")
    sp_count = lax.axis_size("sp")
    lane = lax.axis_index("tp")
    own = tokens // lanes
    model_width = resid.shape[1]
    part = model_width // lanes

    positions = lax.axis_index("sp") * tokens + jnp.arange(tokens, dtype=jnp.int32)
    rotated_keys = apply_rotary_heads(keys.reshape(tokens, 1, width), key_norm_gain, positions)
    both = jnp.concatenate([rotated_keys.reshape(tokens, width), values], 1)
    gates_own = (
        group_weight[:, None] * expert_weight / jnp.sum(expert_weight, -1, keepdims=True)
    )
    top = expert_ids.shape[1]
    sp = lax.axis_index("sp")
    flat = expert_ids.reshape(-1)
    one_hot = (flat[:, None] == jnp.arange(sp_count, dtype=jnp.int32)).astype(jnp.int32)
    earlier = jnp.cumsum(one_hot, 0) - one_hot
    rank = jnp.sum(earlier * one_hot, 1)
    dz = (flat // (2 * X_SIZE) - sp // (2 * X_SIZE)) % Z_SIZE
    dx = (flat // 2 - sp // 2) % X_SIZE
    dc = (flat - sp) % 2
    near = jnp.where(dz <= Z_SIZE // 2, 2 * dz - 2, 2 * (Z_SIZE - dz) - 1)
    near = jnp.where(dz == 0, Z_SIZE - 1, near)
    target = ((near * X_SIZE + dx) * 2 + dc) * 8
    place = lane * CAP + rank
    row_a = jnp.where(place < 8, target + place, -1)
    row_b = jnp.where(place < 8, -1, target + place - 8)
    row_c = jnp.where(place < 8, -1, target + place - 4)
    info = jnp.concatenate(
        [v.reshape(own, top).astype(jnp.float32) for v in (row_a, row_b, row_c)]
        + [gates_own, jnp.zeros((own, 128 - 4 * top), jnp.float32)],
        1,
    )

    q_rot = apply_rotary_heads(queries.reshape(tokens, heads, width), q_gain, positions)
    factor = np.float32(np.log2(np.e) * width**-0.5)
    scaled = q_rot.astype(jnp.float32) * factor
    coarse = lax.reduce_precision(scaled, 8, 7)
    fine = (scaled - coarse).astype(jnp.bfloat16)
    pair = jnp.concatenate([coarse.astype(jnp.bfloat16), fine], -1)
    q_t = pair.transpose(2, 1, 0).reshape(2 * width, heads * tokens)
    x_one, down_slice, table = front(
        q_t, both, out_weight, down_proj[0], resid, info, norm1_gain[None]
    )
    return moe_layer(
        x_one,
        table.reshape(tokens, -1),
        norm2_gain[None],
        gate_proj[0],
        up_proj[0],
        down_slice.reshape(-1, part),
    )


def solution(mesh):
    in_specs = (
        P(("sp", "tp"), None),
        P("sp", "tp"),
        P("sp", "tp"),
        P("sp", "tp"),
        P(),
        P(),
        P("tp", None),
        P(),
        P(),
        P(("sp", "tp"), None),
        P(("sp", "tp")),
        P(("sp", "tp"), None),
        P("sp", None, "tp"),
        P("sp", None, "tp"),
        P("sp", "tp", None),
    )
    out_specs = P(("sp", "tp"), None)
    return jax.shard_map(
        per_device, mesh=mesh, in_specs=in_specs, out_specs=out_specs, check_vma=False
    )
```
